256 devices in a mesh: ep: 64 (over z, y, core), tp: 4 (over x).
Axes of the slice: x: 4, y: 4, z: 8, core: 2. Of those that a mesh axis runs over, the one named last changes fastest.
Arguments:
- queries: bfloat16 [32768, 512], P('ep', 'tp'), may hold values from -6 to 6
- key_rows: bfloat16 [32768, 512], P('ep', 'tp'), may hold values from -6 to 6
- value_rows: bfloat16 [32768, 1024], P('ep', 'tp'), may hold values from -6 to 6
- forget_gate_input: bfloat16 [32768, 512], P('ep', 'tp'), may hold values from -6 to 6
- channel_decay_rate: float32 [512], P('tp'), may hold values from 0 to 1, as said below
- position_decay_factor: float32 [32768], P('ep'), may hold values from 0 to 3, as said below
- extra_log_decay: float32 [32768, 8], P('ep', 'tp'), may hold values from -1 to 0, as said below
- head_norm_gain: float32 [8, 128], P('tp'), may hold values from 0.1 to 1.9
- output_projection_weight: bfloat16 [1024, 2048], P('tp'), may hold values from -0.1875 to 0.1875
- expert_input_rows: bfloat16 [16384, 2048], P('ep'), may hold values from -6 to 6
- expert_norm_gain: float32 [2048], replicated, may hold values from 0.1 to 1.9
- routes: int32 [16384, 2], P('ep'), may hold values from 0 to 63, all different within a row; in each aligned block of 256 rows (0 to 255, 256 to 511, ...) at most 16 rows name the same one
- chosen_expert_weights: float32 [16384, 2], P('ep'), may hold values from 0.2 to 1
- expert_gate_weight: bfloat16 [64, 2048, 3072], P('ep', None, 'tp'), may hold values from -0.125 to 0.125
- expert_up_weight: bfloat16 [64, 2048, 3072], P('ep', None, 'tp'), may hold values from -0.125 to 0.125
- expert_down_weight: bfloat16 [64, 3072, 2048], P('ep', 'tp'), may hold values from -0.109375 to 0.109375
Outputs:
- token_mixer_output: bfloat16 [32768, 2048], P(('ep', 'tp'))
- moe_out: bfloat16 [16384, 2048], P('ep', 'tp')
The draws below stay inside these ranges and needn't reach their ends.
Inputs may be any that keep to these rules, and one draw needn't show every extreme that they name: `routes`: within the rows of one device no expert is named by more than 16 of the choices, a bound that some block reaches; the 2 experts of a token differ. `channel_decay_rate`: Positive. `position_decay_factor`: Positive. `extra_log_decay`: zero or negative.
All inputs are finite; a program needn't handle non-finite values.
Results may differ from the reference program's by a relative error of at most 0.019.
Values may be sent and summed in bfloat16 or wider, within the bound.
A program may use at most 128 MiB of HBM per device.

```python
import math
import jax
import jax.numpy as jnp
import numpy as np
from jax import lax

D = 2048
HEAD_TOTAL = 8
KEY_CHANNELS = 64
VALUE_DIM = 128
SPAN = 64
FF = 3072
TOPK = 2
TOK_EP = 512
TOK_MOE = 256
TOKENS_MIX = 32768
TOKENS_MOE = 16384
EXPERTS = 64
CAPACITY = 16
N_EP = 64
N_TP = 4


def draw_channel_decay_rate(key, part):
    keys_list = jax.random.split(jax.random.fold_in(key, 11), 3)
    slow_share = 0.5
    slow_heads = jax.random.uniform(keys_list[0], (HEAD_TOTAL,)) < slow_share
    slow_rates = jnp.exp(jax.random.uniform(keys_list[1], (HEAD_TOTAL, KEY_CHANNELS), minval=jnp.log(0.2), maxval=0.0)) / TOKENS_MIX
    fast_rates = jnp.exp(jax.random.uniform(keys_list[2], (HEAD_TOTAL, KEY_CHANNELS), minval=jnp.log(0.03), maxval=jnp.log(0.12)))
    return jnp.where(slow_heads[:, None], slow_rates, fast_rates).reshape(HEAD_TOTAL * KEY_CHANNELS).astype(jnp.float32)


def draw_position_decay_factor(key, part):
    block_key, position_key = jax.random.split(jax.random.fold_in(key, 23))
    blocks = TOKENS_MIX // TOK_EP
    block_scale = jnp.exp(jax.random.uniform(block_key, (blocks,), minval=-0.7, maxval=0.7))
    jitter = jnp.exp(jax.random.uniform(position_key, (TOKENS_MIX,), minval=-0.35, maxval=0.35))
    return (jnp.repeat(block_scale, TOK_EP) * jitter).astype(jnp.float32)


def draw_extra_log_decay(key, part):
    where_key, depth_key = jax.random.split(jax.random.fold_in(key, 37))
    struck = jax.random.uniform(where_key, (TOKENS_MIX, HEAD_TOTAL)) < 3.0 / TOKENS_MIX
    depth = jax.random.uniform(depth_key, (TOKENS_MIX, HEAD_TOTAL), minval=-0.6, maxval=-0.2)
    return jnp.where(struck, depth, 0.0).astype(jnp.float32)


def steps_of(rng, extent, cuts, low, largest):
    def one(position, blocks):
        heights = jax.random.uniform(jax.random.fold_in(jax.random.fold_in(rng, 6), position), (blocks,), jnp.float32, low / len(cuts), largest / len(cuts))
        return jnp.repeat(jnp.exp(heights), extent[position] // blocks).reshape((-1,) + (1,) * (len(extent) - position - 1))

    factor_of = one(*cuts[0])
    for cut in cuts[1:]:
        factor_of = factor_of * one(*cut)
    return factor_of


def shared_out(key, own, number, rows, amount, top, reach, lean):
    order = jax.random.permutation(key, amount)
    heavy_load, usual = load_shares(amount, rows * top, reach, lean, True), load_shares(amount, rows * top, reach, lean, False)
    places = jnp.arange(amount)

    def named(tallies, offset_by):
        used = int((tallies > 0).sum())
        fixed = max(1, used // 4)
        moved = fixed + (places - fixed + offset_by * (used - fixed)) % max(1, amount - fixed)
        return jnp.zeros((amount,), jnp.int32).at[order[jnp.where(places < fixed, places, moved)]].set(jnp.asarray(tallies, jnp.int32))

    tallies = jnp.where(number % 4 == 0, named(heavy_load, number // 4), named(usual, number - number // 4 - 1))
    mixed = jax.random.permutation(jax.random.fold_in(own, 3), amount)
    donor, sink = mixed[0:amount // 2 * 2:2], mixed[1:amount // 2 * 2:2]
    room = jnp.minimum(tallies[donor] - 1, reach - tallies[sink]) // 2
    room = jnp.where((donor == order[0]) | (sink == order[0]) | (tallies[sink] == 0), 0, jnp.maximum(room, 0))
    moved = jax.random.randint(jax.random.fold_in(own, 4), (amount // 2,), 0, 1 << 20) % (room + 1)
    tallies = tallies.at[donor].add(-moved).at[sink].add(moved)
    items = jnp.searchsorted(jnp.cumsum(tallies), jnp.arange(rows * top), side="right").astype(jnp.int32)
    grid = items.reshape(top, rows).T
    grid = grid[jax.random.permutation(jax.random.fold_in(own, 1), rows)]
    offset_by = jax.random.randint(jax.random.fold_in(own, 2), (rows, 1), 0, top)
    return jnp.take_along_axis(grid, (jnp.arange(top)[None, :] + offset_by) % top, axis=1)


def load_shares(number_of, total, limit, lean, full):
    loads = [(1 << 20) // math.isqrt(rank ** lean) + 1 for rank in range(1, number_of + 1)]
    largest = limit if full else min(limit, max(-(-total // number_of), total * loads[0] // sum(loads)))
    least = 1 if total - largest >= number_of - 1 else 0
    counts, rest = [largest] + [least] * (number_of - 1), total - largest - least * (number_of - 1)
    while rest > 0:
        free = [i for i in range(1, number_of) if counts[i] < largest] or [i for i in range(1, number_of) if counts[i] < limit]
        pool, budget = sum([loads[i] for i in free]), rest
        for i in free:
            more = min(limit - counts[i], max(1, budget * loads[i] // pool), rest)
            counts[i] = counts[i] + more
            rest = rest - more
    return np.array(counts)


def centred(key, extent, spread, reach, shards=(), kind=jnp.bfloat16):
    result = spread * jax.random.normal(key, extent, jnp.float32)
    if shards:
        result = result * steps_of(key, extent, shards, -0.22, 0.18)
    return jnp.clip(result, -reach, reach).astype(kind)


def setup_inputs(seed: int = 0) -> dict:
    seeds = jax.random.split(jax.random.key(seed), 17)
    queries = centred(seeds[0], (TOKENS_MIX, HEAD_TOTAL * KEY_CHANNELS), 1.0, 6.0, ((0, 64), (1, 4)))
    key_rows = centred(seeds[1], (TOKENS_MIX, HEAD_TOTAL * KEY_CHANNELS), 1.0, 6.0, ((0, 64), (1, 4)))
    value_rows = centred(seeds[2], (TOKENS_MIX, HEAD_TOTAL * VALUE_DIM), 1.0, 6.0, ((0, 64), (1, 4)))
    forget_gate_input = centred(seeds[3], (TOKENS_MIX, HEAD_TOTAL * KEY_CHANNELS), 1.5, 6.0, ((0, 64), (1, 4)))
    channel_decay_rate = draw_channel_decay_rate(jax.random.fold_in(seeds[16], 71), 0)
    position_decay_factor = draw_position_decay_factor(jax.random.fold_in(seeds[16], 71), 0)
    extra_log_decay = draw_extra_log_decay(jax.random.fold_in(seeds[16], 71), 0)
    head_norm_gain = jnp.clip(1.0 + 0.18 * jax.random.normal(seeds[7], (HEAD_TOTAL, VALUE_DIM), jnp.float32), 0.1, 1.9)
    output_projection_weight = centred(seeds[8], (HEAD_TOTAL * VALUE_DIM, D), (HEAD_TOTAL * VALUE_DIM) ** -0.5, 0.1875, ((0, 4),))
    expert_input_rows = centred(seeds[9], (TOKENS_MOE, D), 1.0, 6.0, ((0, 64),))
    expert_norm_gain = jnp.clip(1.0 + 0.18 * jax.random.normal(seeds[10], (D,), jnp.float32), 0.1, 1.9)
    routes_keys = jax.random.split(jax.random.fold_in(seeds[11], 1), TOKENS_MOE // TOK_MOE)
    routes_turns = jax.random.permutation(jax.random.fold_in(seeds[11], 3), TOKENS_MOE // TOK_MOE)
    routes = jax.vmap(lambda own, number: shared_out(jax.random.fold_in(seeds[11], 2), own, number, TOK_MOE, EXPERTS, TOPK, CAPACITY, 1))(routes_keys, routes_turns).reshape((TOKENS_MOE, TOPK))
    chosen_expert_weights = jnp.clip(0.2 + 0.8 * jax.random.uniform(seeds[12], (TOKENS_MOE, TOPK), jnp.float32) ** steps_of(seeds[12], (TOKENS_MOE, TOPK), ((0, 64),), -0.2, 0.2), 0.2, 1.0)
    expert_gate_weight = centred(seeds[13], (EXPERTS, D, FF), D ** -0.5, 0.125, ((0, 64), (2, 4)))
    expert_up_weight = centred(seeds[14], (EXPERTS, D, FF), D ** -0.5, 0.125, ((0, 64), (2, 4)))
    expert_down_weight = centred(seeds[15], (EXPERTS, FF, D), FF ** -0.5, 0.109375, ((0, 64), (1, 4)))
    return dict(queries=queries, key_rows=key_rows, value_rows=value_rows, forget_gate_input=forget_gate_input, channel_decay_rate=channel_decay_rate, position_decay_factor=position_decay_factor, extra_log_decay=extra_log_decay, head_norm_gain=head_norm_gain, output_projection_weight=output_projection_weight, expert_input_rows=expert_input_rows, expert_norm_gain=expert_norm_gain, routes=routes, chosen_expert_weights=chosen_expert_weights, expert_gate_weight=expert_gate_weight, expert_up_weight=expert_up_weight, expert_down_weight=expert_down_weight)


highest_precision = lax.Precision.HIGHEST
norm_eps = 1e-06

def gla_blocks(query_single, key_float, value_float, decay_logarithm, span_rows):
    length, head_count, key_width = query_single.shape
    value_width = value_float.shape[-1]
    block_count = length // span_rows

    def blocked(tensor):
        return tensor.reshape(block_count, span_rows, head_count, tensor.shape[-1])
    causal = (jnp.arange(span_rows)[:, None] >= jnp.arange(span_rows)[None, :])[:, :, None, None]

    def advance(carried_state, pieces):
        block_queries, block_keys, block_values, gate_block = pieces
        cumulative_decay = jnp.cumsum(gate_block, axis=0)
        log_gaps = cumulative_decay[:, None] - cumulative_decay[None, :]
        decays = jnp.exp(jnp.where(causal, log_gaps, -jnp.inf))
        scores = lax.optimization_barrier(jnp.sum(block_queries[:, None] * block_keys[None, :] * decays, axis=-1))
        final_output = jnp.einsum('ijh,jhv->ihv', scores, block_values, precision=highest_precision)
        final_output = final_output + jnp.einsum('nwt,wto->nwo', block_queries * jnp.exp(cumulative_decay), carried_state, precision=highest_precision)
        final_log_decay = cumulative_decay[-1]
        carried_state = jnp.exp(final_log_decay)[:, :, None] * carried_state + jnp.einsum('ygc,yga->gca', block_keys * jnp.exp(final_log_decay[None] - cumulative_decay), block_values, precision=highest_precision)
        return (carried_state, final_output)
    start_state = jnp.zeros((head_count, key_width, value_width), jnp.float32)
    carried_state, outputs = lax.scan(advance, start_state, (blocked(query_single), blocked(key_float), blocked(value_float), blocked(decay_logarithm)))
    return (outputs.reshape(length, head_count, value_width), carried_state)

def reference_mixer(queries, key_rows, value_rows, forget_gate_input, channel_decay_rate, position_decay_factor, extra_log_decay, head_norm_gain, output_projection_weight):
    length = queries.shape[0]
    query_single = queries.astype(jnp.float32).reshape(length, HEAD_TOTAL, KEY_CHANNELS)
    key_float = key_rows.astype(jnp.float32).reshape(length, HEAD_TOTAL, KEY_CHANNELS)
    value_float = value_rows.astype(jnp.float32).reshape(length, HEAD_TOTAL, VALUE_DIM)
    gate_logarithm = jax.nn.log_sigmoid(forget_gate_input.astype(jnp.float32)).reshape(length, HEAD_TOTAL, KEY_CHANNELS)
    decay_logarithm = gate_logarithm * channel_decay_rate.reshape(HEAD_TOTAL, KEY_CHANNELS)[None] * position_decay_factor[:, None, None] + extra_log_decay[:, :, None]
    mixed_out, unused = gla_blocks(query_single, key_float, value_float, decay_logarithm, SPAN)
    scale = lax.rsqrt(lax.optimization_barrier(jnp.mean(mixed_out * mixed_out, axis=-1, keepdims=True)) + norm_eps)
    head_normed = (mixed_out * scale * head_norm_gain[None]).astype(jnp.bfloat16).reshape(length, HEAD_TOTAL * VALUE_DIM)
    group_width = HEAD_TOTAL * VALUE_DIM // N_TP
    running = jnp.zeros((length, D), jnp.float32)
    for member in range(N_TP):
        partial_value = jnp.dot(head_normed[:, member * group_width:(member + 1) * group_width], output_projection_weight[member * group_width:(member + 1) * group_width], preferred_element_type=jnp.float32).astype(jnp.bfloat16)
        running = running + lax.optimization_barrier(partial_value).astype(jnp.float32)
    return running.astype(jnp.bfloat16)

def expert_reference(expert_input_rows, expert_norm_gain, routes, chosen_expert_weights, expert_gate_weight, expert_up_weight, expert_down_weight):
    rows_float = expert_input_rows.astype(jnp.float32)
    scaled = rows_float * lax.rsqrt(lax.optimization_barrier(jnp.mean(rows_float * rows_float, axis=-1, keepdims=True)) + norm_eps)
    moe_normed = (scaled * expert_norm_gain[None]).astype(jnp.bfloat16)
    flat_routes = routes.reshape(-1)
    flat_weights = chosen_expert_weights.reshape(-1)
    slot_total = N_EP * CAPACITY
    group_width = FF // N_TP

    def one_expert(accumulator, inputs):
        gate_weight, up_weight, down_weight, expert_id = inputs
        routed_here = flat_routes == expert_id
        picked = jnp.nonzero(routed_here, size=slot_total, fill_value=0)[0].astype(jnp.int32)
        live_slot = (jnp.arange(slot_total, dtype=jnp.int32) < jnp.sum(routed_here.astype(jnp.int32))).astype(jnp.float32)
        token_rows = (picked // TOPK).astype(jnp.int32)
        chosen = moe_normed[token_rows]
        gate_sum = jnp.dot(chosen, gate_weight, preferred_element_type=jnp.float32)
        up_sum = jnp.dot(chosen, up_weight, preferred_element_type=jnp.float32)
        hidden = (jax.nn.silu(gate_sum) * up_sum).astype(jnp.bfloat16)
        running = jnp.zeros((slot_total, D), jnp.float32)
        for member in range(N_TP):
            partial_value = jnp.dot(hidden[:, member * group_width:(member + 1) * group_width], down_weight[member * group_width:(member + 1) * group_width], preferred_element_type=jnp.float32).astype(jnp.bfloat16)
            running = running + lax.optimization_barrier(partial_value).astype(jnp.float32)
        expert_result = lax.optimization_barrier(running.astype(jnp.bfloat16)).astype(jnp.float32)
        weighted = expert_result * (flat_weights[picked] * live_slot)[:, None]
        return (accumulator.at[token_rows].add(weighted), None)
    empty_sum = jnp.zeros((TOKENS_MOE, D), jnp.float32)
    combined, unused = lax.scan(one_expert, empty_sum, (expert_gate_weight, expert_up_weight, expert_down_weight, jnp.arange(EXPERTS, dtype=jnp.int32)))
    return combined.astype(jnp.bfloat16)

def reference(queries, key_rows, value_rows, forget_gate_input, channel_decay_rate, position_decay_factor, extra_log_decay, head_norm_gain, output_projection_weight, expert_input_rows, expert_norm_gain, routes, chosen_expert_weights, expert_gate_weight, expert_up_weight, expert_down_weight):
    token_mixer_output = reference_mixer(queries, key_rows, value_rows, forget_gate_input, channel_decay_rate, position_decay_factor, extra_log_decay, head_norm_gain, output_projection_weight)
    moe_out = expert_reference(expert_input_rows, expert_norm_gain, routes, chosen_expert_weights, expert_gate_weight, expert_up_weight, expert_down_weight)
    return (token_mixer_output, moe_out)
```

```python
import functools

import jax
import jax.numpy as jnp
from jax import lax
from jax.experimental import pallas as pl
from jax.experimental.pallas import tpu as pltpu
from jax.sharding import Mesh
from jax.sharding import PartitionSpec as P

F32, BF16 = jnp.float32, jnp.bfloat16
MESH = pl.DeviceIdType.MESH
NX = 4
CAP = 16
BLOCK = 128
LEVELS = (64, 32, 16, 8, 4, 2, 1)
EPS = 1e-06
EP = ("z", "yc")
EP_TP = ("z", "yc", "tp")


def dot(a, b):
    return jnp.dot(a, b, preferred_element_type=F32)


def dot_nt(a, b):
    return lax.dot_general(a, b, (((1,), (1,)), ((), ())), preferred_element_type=F32)


def dot_tn(a, b):
    return lax.dot_general(a, b, (((0,), (0,)), ((), ())), preferred_element_type=F32)


def iota(shape, dim):
    return lax.broadcasted_iota(jnp.int32, shape, dim)


def one_where(mask):
    return jnp.where(mask, 1.0, 0.0)


def away_order(count):
    order = [0]
    for d in range(1, count // 2 + 1):
        for e in (d, count - d):
            if e not in order:
                order.append(e)
    return order


def kernel(
    nz,
    nyc,
    per_chunk,
    routes,
    routes_t,
    chosen,
    rows,
    gain,
    queries,
    keys,
    values,
    log_decay,
    head_gain,
    out_weight,
    gate_hbm,
    up_hbm,
    down_hbm,
    mix_out,
    moe_out,
    gate_w,
    up_w,
    down_w,
    weight_sem,
    zsnd,
    zin,
    xq,
    part,
    pass_a,
    pass_b,
    from_left,
    from_right,
    result,
    yin,
    zret,
    zs,
    zr,
    ys,
    yr,
    xs,
    xr,
    ps,
    pr,
    y2s,
    y2r,
    z2s,
    z2r,
    sums,
    local_out,
    decayed_q,
    state,
    total,
    normed,
    sy,
    tz,
    sz,
    incoming,
    before,
    sys_,
    syr,
    szs,
    szr,
    mp,
    mpa,
    mpb,
    mq1,
    mq3,
    ms,
    mr,
):
    z, yc, x = lax.axis_index("z"), lax.axis_index("yc"), lax.axis_index("tp")
    right, left = lax.rem(x + 1, NX), lax.rem(x + NX - 1, NX)
    order = away_order(nz)
    zrows = nyc * CAP
    half = zrows // 2
    quarter = rows.shape[1] // NX
    tokens = rows.shape[0]
    length = queries.shape[0]
    blocks = length // BLOCK
    chunks = nz // per_chunk
    crows = per_chunk * zrows

    def remote(src, dst, send, recv, device):
        return pltpu.make_async_remote_copy(
            src_ref=src, dst_ref=dst, send_sem=send, recv_sem=recv, device_id=device, device_id_type=MESH
        )

    def arrived(ref, sem):
        pltpu.make_async_copy(ref, ref, sem).wait()

    def times(value, unit):
        return pl.multiple_of(value * unit, unit)

    def columns(r):
        return pl.ds(r * quarter, quarter)

    loads = []
    for r in range(NX):
        back = times(lax.rem(x + NX - r, NX), quarter)
        ahead = times(lax.rem(x + r, NX), quarter)
        loads += [
            pltpu.make_async_copy(gate_hbm.at[0, pl.ds(back, quarter), :], gate_w.at[columns(r), :], weight_sem.at[3 * r]),
            pltpu.make_async_copy(up_hbm.at[0, pl.ds(back, quarter), :], up_w.at[columns(r), :], weight_sem.at[3 * r + 1]),
            pltpu.make_async_copy(down_hbm.at[0, :, pl.ds(ahead, quarter)], down_w.at[:, columns(r)], weight_sem.at[3 * r + 2]),
        ]
    for load in loads:
        load.start()

    barrier = pltpu.get_barrier_semaphore()
    pl.semaphore_signal(barrier, inc=1, device_id={"tp": right}, device_id_type=MESH)
    pl.semaphore_signal(barrier, inc=1, device_id={"tp": left}, device_id_type=MESH)

    def greet_z(t, carry):
        pl.semaphore_signal(barrier, inc=1, device_id={"z": lax.rem(z + t, nz)}, device_id_type=MESH)
        return carry

    def greet_y(t, carry):
        pl.semaphore_signal(barrier, inc=1, device_id={"yc": lax.rem(yc + t, nyc)}, device_id_type=MESH)
        return carry

    lax.fori_loop(1, nz, greet_z, 0)
    lax.fori_loop(1, nyc, greet_y, 0)

    experts = nz * nyc
    first_t, second_t = routes_t[0:1, :], routes_t[1:2, :]
    marks = [one_where(iota((experts, tokens), 0) == e) for e in (first_t, second_t)]
    upper = one_where(iota((tokens, tokens), 0) < iota((tokens, tokens), 1)).astype(BF16)
    ranks = [dot(m.astype(BF16), upper) for m in marks]
    ranks[1] = ranks[1] + jnp.sum(marks[0], axis=1, keepdims=True)
    slots_t = [
        e.astype(F32) * CAP + jnp.sum(m * r, axis=0, keepdims=True)
        for e, m, r in zip((first_t, second_t), marks, ranks)
    ]

    own = times(x, quarter)
    squares = rows[...].astype(F32)
    scale = lax.rsqrt(jnp.mean(squares * squares, axis=1, keepdims=True) + EPS)
    moe_normed = (rows[:, pl.ds(own, quarter)].astype(F32) * scale * gain[:, pl.ds(own, quarter)]).astype(BF16)

    pl.semaphore_wait(barrier, 2 + (nz - 1) + (nyc - 1))

    for k, d in enumerate(order):
        base = lax.rem(z + d, nz) * zrows
        slot = (iota((zrows, tokens), 0) + base).astype(F32)
        chooser = one_where((slot == slots_t[0]) | (slot == slots_t[1])).astype(BF16)
        zsnd[k] = dot(chooser, moe_normed).astype(BF16)
        if k:
            remote(zsnd.at[k], zin.at[k], zs.at[k], zr.at[k], {"z": lax.rem(z + d, nz)}).start()

    def forward_y(k):
        source = zin if k else zsnd
        if k:
            arrived(zin.at[k], zr.at[k])

        def send(t, carry):
            to = lax.rem(yc + t, nyc)
            remote(
                source.at[k, pl.ds(times(to, CAP), CAP), :],
                xq.at[pl.ds(pl.multiple_of(k * zrows + yc * CAP, CAP), CAP), columns(0)],
                ys.at[k],
                yr.at[k],
                {"yc": to},
            ).start()
            return carry

        lax.fori_loop(1, nyc, send, 0)
        xq[pl.ds(pl.multiple_of(k * zrows + yc * CAP, CAP), CAP), columns(0)] = source[k, pl.ds(times(yc, CAP), CAP), :]

    def forward_x(k):
        mine = xq.at[pl.ds(k * zrows, zrows), columns(0)]
        arrived(xq.at[pl.ds(k * zrows, zrows - CAP), columns(0)], yr.at[k])
        remote(mine, xq.at[pl.ds(k * zrows, zrows), columns(1)], xs.at[0, k], xr.at[0, k], {"tp": right}).start()
        remote(mine, xq.at[pl.ds(k * zrows, zrows), columns(3)], xs.at[1, k], xr.at[1, k], {"tp": left}).start()

    def relay(k):
        a, b = pl.ds(k * zrows, half), pl.ds(k * zrows + half, half)
        arrived(xq.at[pl.ds(k * zrows, zrows), columns(1)], xr.at[0, k])
        remote(xq.at[a, columns(1)], xq.at[a, columns(2)], xs.at[2, k], xr.at[2, k], {"tp": right}).start()
        arrived(xq.at[pl.ds(k * zrows, zrows), columns(3)], xr.at[1, k])
        remote(xq.at[b, columns(3)], xq.at[b, columns(2)], xs.at[3, k], xr.at[3, k], {"tp": left}).start()

    chalf = crows // 2

    def expert(c):
        for k in range(c * per_chunk, (c + 1) * per_chunk):
            arrived(xq.at[pl.ds(k * zrows, half), columns(2)], xr.at[2, k])
            arrived(xq.at[pl.ds(k * zrows + half, half), columns(2)], xr.at[3, k])
        if c == 0:
            for load in loads:
                load.wait()
        here = pl.ds(c * crows, crows)
        gate = dot(xq[here, :], gate_w[...])
        up = dot(xq[here, :], up_w[...])
        hidden = (jax.nn.silu(gate) * up).astype(BF16)
        part[here, :] = dot(hidden, down_w[...]).astype(BF16)
        a, b = pl.ds(c * crows, chalf), pl.ds(c * crows + chalf, chalf)
        remote(part.at[a, columns(2)], pass_a.at[c], ps.at[0, c], pr.at[0, c], {"tp": right}).start()
        remote(part.at[b, columns(2)], pass_b.at[c], ps.at[1, c], pr.at[1, c], {"tp": left}).start()

    def add_pass(c):
        here = pl.ds(c * crows, crows)
        a, b = pl.ds(c * crows, chalf), pl.ds(c * crows + chalf, chalf)
        arrived(pass_a.at[c], pr.at[0, c])
        part[a, columns(1)] = (part[a, columns(1)].astype(F32) + pass_a[c].astype(F32)).astype(BF16)
        remote(part.at[here, columns(1)], from_left.at[here], ps.at[2, c], pr.at[2, c], {"tp": right}).start()
        arrived(pass_b.at[c], pr.at[1, c])
        part[b, columns(3)] = (part[b, columns(3)].astype(F32) + pass_b[c].astype(F32)).astype(BF16)
        remote(part.at[here, columns(3)], from_right.at[here], ps.at[3, c], pr.at[3, c], {"tp": left}).start()

    def give_back_y(c):
        here = pl.ds(c * crows, crows)
        arrived(from_left.at[here], pr.at[2, c])
        arrived(from_right.at[here], pr.at[3, c])
        result[here, :] = (
            part[here, columns(0)].astype(F32) + from_left[here, :].astype(F32) + from_right[here, :].astype(F32)
        ).astype(BF16)
        for k in range(c * per_chunk, (c + 1) * per_chunk):

            def send(t, carry):
                to = lax.rem(yc + t, nyc)
                remote(
                    result.at[pl.ds(pl.multiple_of(k * zrows + to * CAP, CAP), CAP), :],
                    yin.at[k, pl.ds(times(yc, CAP), CAP), :],
                    y2s.at[k],
                    y2r.at[k],
                    {"yc": to},
                ).start()
                return carry

            lax.fori_loop(1, nyc, send, 0)
            yin[k, pl.ds(times(yc, CAP), CAP), :] = result[pl.ds(pl.multiple_of(k * zrows + yc * CAP, CAP), CAP), :]

    def give_back_z(c):
        for k in range(c * per_chunk, (c + 1) * per_chunk):
            arrived(yin.at[k, pl.ds(0, zrows - CAP), :], y2r.at[k])
            if k:
                to = lax.rem(z + nz - order[k], nz)
                remote(yin.at[k], zret.at[k], z2s.at[k], z2r.at[k], {"z": to}).start()

    def combine():
        first, second = routes[:, 0:1], routes[:, 1:2]
        marks = [one_where(iota((tokens, experts), 1) == e) for e in (first, second)]
        lower = one_where(iota((tokens, tokens), 0) > iota((tokens, tokens), 1)).astype(BF16)
        ranks = [dot(lower, m.astype(BF16)) for m in marks]
        ranks[1] = ranks[1] + jnp.sum(marks[0], axis=0, keepdims=True)
        slots = [
            e.astype(F32) * CAP + jnp.sum(m * r, axis=1, keepdims=True)
            for e, m, r in zip((first, second), marks, ranks)
        ]
        mixed = jnp.zeros((tokens, quarter), F32)
        for k, d in enumerate(order):
            base = lax.rem(z + d, nz) * zrows
            slot = (iota((tokens, zrows), 1) + base).astype(F32)
            weight = jnp.where(slot == slots[0], chosen[:, 0:1], 0.0) + jnp.where(slot == slots[1], chosen[:, 1:2], 0.0)
            high = weight.astype(BF16)
            low = (weight - high.astype(F32)).astype(BF16)
            if k:
                arrived(zret.at[k], z2r.at[k])
            returned = zret[k] if k else yin[k]
            mixed = mixed + dot(high, returned) + dot(low, returned)
        moe_out[...] = mixed.astype(BF16)

    def prepare_sums():
        i, j = iota((BLOCK, BLOCK), 0), iota((BLOCK, BLOCK), 1)
        for level, h in enumerate(LEVELS):
            edge = (i & ~(2 * h - 1)) + h
            after = (j >= edge) & (j <= i)
            ahead = (j > i) & (j < edge)
            m = one_where(after | ahead).astype(BF16)
            sums[pl.ds(level * BLOCK, BLOCK), pl.ds(0, BLOCK)] = m
            sums[pl.ds(level * BLOCK, BLOCK), pl.ds(BLOCK, BLOCK)] = m
        for level, m in ((len(LEVELS), j <= i), (len(LEVELS) + 1, j > i)):
            m = one_where(m).astype(BF16)
            sums[pl.ds(level * BLOCK, BLOCK), pl.ds(0, BLOCK)] = m
            sums[pl.ds(level * BLOCK, BLOCK), pl.ds(BLOCK, BLOCK)] = m

    first_head = iota((BLOCK, BLOCK), 1) < BLOCK // 2

    def by_head(value):
        return jnp.concatenate([jnp.where(first_head, value, 0.0), jnp.where(first_head, 0.0, value)], axis=0).astype(BF16)

    def gla_block(b):
        r = pl.ds(b * BLOCK, BLOCK)
        g = log_decay[r, :]
        high = g.astype(BF16)
        low = (g - high.astype(F32)).astype(BF16)
        e = jnp.exp(dot(sums[...], jnp.concatenate([high, low], axis=0)))
        q, k = queries[r, :].astype(F32), keys[r, :].astype(F32)
        i, j = iota((BLOCK, 2 * BLOCK), 0), iota((BLOCK, 2 * BLOCK), 1) & (BLOCK - 1)
        apart = i ^ j
        scores = None
        for level, h in enumerate(LEVELS):
            factor = e[level * BLOCK : (level + 1) * BLOCK]
            s = dot_nt((q * factor).astype(BF16), by_head(k * factor))
            scores = s if scores is None else jnp.where(apart < 2 * h, s, scores)
        scores = jnp.where(apart < 1, dot_nt(queries[r, :], by_head(k)), scores)
        scores = jnp.where(i >= j, scores, 0.0).astype(BF16)
        n = len(LEVELS)
        from_start = e[n * BLOCK : (n + 1) * BLOCK]
        to_end = e[(n + 1) * BLOCK : (n + 2) * BLOCK]
        qg = q * from_start
        outs = [
            dot(scores[:, h * BLOCK : (h + 1) * BLOCK], values[r, pl.ds(h * BLOCK, BLOCK)]) for h in range(2)
        ]
        if b:
            carried = dot_nt(by_head(qg), state[...].astype(BF16))
            outs = [o + carried[h * BLOCK : (h + 1) * BLOCK] for h, o in enumerate(outs)]
            decayed_q[r, :] = (qg * total[...]).astype(BF16)
        else:
            decayed_q[r, :] = qg.astype(BF16)
        for h in range(2):
            local_out[r, pl.ds(h * BLOCK, BLOCK)] = outs[h]
        grown = dot_tn(values[r, :], (k * to_end).astype(BF16))
        fresh = jnp.where(first_head, grown[0:BLOCK], grown[BLOCK : 2 * BLOCK])
        through = from_start[BLOCK - 1 : BLOCK, :]
        if b:
            state[...] = state[...] * through + fresh
            total[...] = total[...] * through
        else:
            state[...] = fresh
            total[...] = through

    def packed(s, d):
        high = d.astype(BF16).astype(F32)
        row = iota((16, BLOCK), 0)
        tail = jnp.where(row == 0, high, jnp.where(row == 1, d - high, 0.0))
        return s.astype(BF16), tail.astype(BF16)

    def opened(ref, at):
        tail = ref[at, pl.ds(BLOCK, 16), :].astype(F32)
        return ref[at, pl.ds(0, BLOCK), :].astype(F32), tail[0:1] + tail[1:2]

    def states_y():
        s, tail = packed(state[...], total[...])
        tz[1, pl.ds(0, BLOCK), :] = s
        tz[1, pl.ds(BLOCK, 16), :] = tail

        def send(t, carry):
            to = lax.rem(yc + t, nyc)
            remote(tz.at[1], sy.at[yc], sys_, syr, {"yc": to}).start()
            return carry

        lax.fori_loop(1, nyc, send, 0)
        sy[yc, pl.ds(0, BLOCK), :] = s
        sy[yc, pl.ds(BLOCK, 16), :] = tail

    def states_z():
        arrived(sy.at[pl.ds(0, nyc - 1)], syr)
        run_s, run_d = jnp.zeros((BLOCK, BLOCK), F32), jnp.ones((1, BLOCK), F32)
        before[pl.ds(0, BLOCK), :] = run_s
        before[pl.ds(BLOCK, 8), :] = jnp.broadcast_to(run_d, (8, BLOCK))
        for s in range(nyc):
            new_s, new_d = opened(sy, s)
            run_s, run_d = run_s * new_d + new_s, run_d * new_d

            @pl.when(s < yc)
            def _(run_s=run_s, run_d=run_d):
                before[pl.ds(0, BLOCK), :] = run_s
                before[pl.ds(BLOCK, 8), :] = jnp.broadcast_to(run_d, (8, BLOCK))

        s, tail = packed(run_s, run_d)
        tz[0, pl.ds(0, BLOCK), :] = s
        tz[0, pl.ds(BLOCK, 16), :] = tail
        for d in range(1, nz):

            @pl.when(z + d < nz)
            def _(d=d):
                remote(tz.at[0], sz.at[z], szs.at[d], szr.at[z], {"z": z + d}).start()

    def states_in():
        incoming[...] = jnp.zeros((BLOCK, BLOCK), F32)
        for s in range(nz - 1):

            @pl.when(s < z)
            def _(s=s):
                arrived(sz.at[s], szr.at[s])
                new_s, new_d = opened(sz, s)
                incoming[...] = incoming[...] * new_d + new_s

        incoming[...] = incoming[...] * before[pl.ds(BLOCK, 8), :][0:1] + before[pl.ds(0, BLOCK), :]

    mrows = length // NX
    mhalf = mrows // 2

    def mix():
        s = incoming[...].astype(BF16)
        for b in range(blocks):
            r = pl.ds(b * BLOCK, BLOCK)
            carried = dot_nt(by_head(decayed_q[r, :].astype(F32)), s)
            for h in range(2):
                c = pl.ds(h * BLOCK, BLOCK)
                o = local_out[r, c] + carried[h * BLOCK : (h + 1) * BLOCK]
                o = o * lax.rsqrt(jnp.mean(o * o, axis=1, keepdims=True) + EPS) * head_gain[h : h + 1, :]
                normed[r, c] = o.astype(BF16)
        for r in (2, 1, 3, 0):
            to = times(lax.rem(x + r, NX), mrows)
            mp[r] = dot(normed[pl.ds(to, mrows), :], out_weight[...]).astype(BF16)
            if r == 2:
                remote(mp.at[2, pl.ds(0, mhalf)], mpa, ms.at[0], mr.at[0], {"tp": right}).start()
                remote(mp.at[2, pl.ds(mhalf, mhalf)], mpb, ms.at[1], mr.at[1], {"tp": left}).start()

    def mix_pass():
        a, b = pl.ds(0, mhalf), pl.ds(mhalf, mhalf)
        arrived(mpa, mr.at[0])
        mp[1, a] = (mp[1, a].astype(F32) + mpa[...].astype(F32)).astype(BF16)
        remote(mp.at[1], mq1, ms.at[2], mr.at[2], {"tp": right}).start()
        arrived(mpb, mr.at[1])
        mp[3, b] = (mp[3, b].astype(F32) + mpb[...].astype(F32)).astype(BF16)
        remote(mp.at[3], mq3, ms.at[3], mr.at[3], {"tp": left}).start()

    def mix_end():
        arrived(mq1, mr.at[2])
        arrived(mq3, mr.at[3])
        mix_out[...] = (mp[0].astype(F32) + mq1[...].astype(F32) + mq3[...].astype(F32)).astype(BF16)

    def step(work, index, count):
        if 0 <= index < count:
            work(index)

    prepare_sums()
    settle = per_chunk + 2
    last = settle + per_chunk * (chunks - 1) + 3
    for s in range(last + 1):
        step(forward_y, s, nz)
        step(forward_x, s - 1, nz)
        step(relay, s - 2, nz)
        for lag, work in ((3, give_back_z), (2, give_back_y), (1, add_pass), (0, expert)):
            at = s - settle - lag
            if at % per_chunk == 0:
                step(work, at // per_chunk, chunks)
        step(gla_block, s, blocks)
        if s == blocks - 1:
            states_y()
        if s == blocks + 1:
            states_z()
        if s == blocks + 3:
            states_in()
            mix()
        if s == blocks + 5:
            mix_pass()
        if s == blocks + 7:
            mix_end()
    if last < blocks + 3:
        states_in()
        mix()
    if last < blocks + 5:
        mix_pass()
    if last < blocks + 7:
        mix_end()
    combine()

    for k in range(nz):
        arrived(xq.at[pl.ds(0, zrows - CAP), columns(0)], ys.at[k])
        arrived(yin.at[0, pl.ds(0, zrows - CAP), :], y2s.at[k])
        if k:
            arrived(zsnd.at[k], zs.at[k])
            arrived(yin.at[k], z2s.at[k])
        for side in range(2):
            arrived(xq.at[pl.ds(0, zrows), columns(0)], xs.at[side, k])
            arrived(xq.at[pl.ds(0, half), columns(0)], xs.at[2 + side, k])
    for c in range(chunks):
        for side in range(2):
            arrived(pass_a.at[c], ps.at[side, c])
            arrived(from_left.at[pl.ds(0, crows)], ps.at[2 + side, c])
    arrived(sy.at[pl.ds(0, nyc - 1)], sys_)
    for d in range(1, nz):

        @pl.when(z + d < nz)
        def _(d=d):
            arrived(tz.at[0], szs.at[d])

    for side in range(2):
        arrived(mpa, ms.at[side])
        arrived(mq1, ms.at[2 + side])


def body(
    nz,
    nyc,
    per_chunk,
    queries,
    key_rows,
    value_rows,
    forget_gate_input,
    channel_decay_rate,
    position_decay_factor,
    extra_log_decay,
    head_norm_gain,
    output_projection_weight,
    expert_input_rows,
    expert_norm_gain,
    routes,
    chosen_expert_weights,
    expert_gate_weight,
    expert_up_weight,
    expert_down_weight,
):
    length, channels = queries.shape
    tokens, width = expert_input_rows.shape
    hidden = expert_gate_weight.shape[2]
    quarter = width // NX
    zrows = nyc * CAP
    crows = per_chunk * zrows
    chunks = nz // per_chunk
    heads = extra_log_decay.shape[1]
    extra = jnp.where(
        lax.broadcasted_iota(jnp.int32, (length, channels), 1) < channels // heads,
        extra_log_decay[:, 0:1],
        extra_log_decay[:, 1:2],
    )
    log_decay = (
        jax.nn.log_sigmoid(forget_gate_input.astype(F32)) * channel_decay_rate[None, :] * position_decay_factor[:, None]
        + extra
    )
    dma, vmem = pltpu.SemaphoreType.DMA, pltpu.VMEM
    mrows = length // NX
    return pl.pallas_call(
        functools.partial(kernel, nz, nyc, per_chunk),
        out_shape=(
            jax.ShapeDtypeStruct((mrows, width), BF16),
            jax.ShapeDtypeStruct((tokens, quarter), BF16),
        ),
        in_specs=[pl.BlockSpec(memory_space=vmem)] * 11 + [pl.BlockSpec(memory_space=pl.ANY)] * 3,
        out_specs=(pl.BlockSpec(memory_space=vmem), pl.BlockSpec(memory_space=vmem)),
        scratch_shapes=[
            vmem((width, hidden), BF16),
            vmem((width, hidden), BF16),
            vmem((hidden, width), BF16),
            dma((3 * NX,)),
            vmem((nz, zrows, quarter), BF16),
            vmem((nz, zrows, quarter), BF16),
            vmem((nz * zrows, width), BF16),
            vmem((nz * zrows, width), BF16),
            vmem((chunks, crows // 2, quarter), BF16),
            vmem((chunks, crows // 2, quarter), BF16),
            vmem((nz * zrows, quarter), BF16),
            vmem((nz * zrows, quarter), BF16),
            vmem((nz * zrows, quarter), BF16),
            vmem((nz, zrows, quarter), BF16),
            vmem((nz, zrows, quarter), BF16),
            dma((nz,)),
            dma((nz,)),
            dma((nz,)),
            dma((nz,)),
            dma((4, nz)),
            dma((4, nz)),
            dma((4, chunks)),
            dma((4, chunks)),
            dma((nz,)),
            dma((nz,)),
            dma((nz,)),
            dma((nz,)),
            vmem(((len(LEVELS) + 2) * BLOCK, 2 * BLOCK), BF16),
            vmem((length, 2 * BLOCK), F32),
            vmem((length, BLOCK), BF16),
            vmem((BLOCK, BLOCK), F32),
            vmem((1, BLOCK), F32),
            vmem((length, 2 * BLOCK), BF16),
            vmem((nyc, BLOCK + 16, BLOCK), BF16),
            vmem((2, BLOCK + 16, BLOCK), BF16),
            vmem((nz, BLOCK + 16, BLOCK), BF16),
            vmem((BLOCK, BLOCK), F32),
            vmem((BLOCK + 8, BLOCK), F32),
            dma(()),
            dma(()),
            dma((nz,)),
            dma((nz,)),
            vmem((NX, mrows, width), BF16),
            vmem((mrows // 2, width), BF16),
            vmem((mrows // 2, width), BF16),
            vmem((mrows, width), BF16),
            vmem((mrows, width), BF16),
            dma((4,)),
            dma((4,)),
        ],
        compiler_params=pltpu.CompilerParams(
            collective_id=0, has_side_effects=True, vmem_limit_bytes=60 * 1024 * 1024
        ),
        name="mixer_and_experts",
    )(
        routes,
        routes.T,
        chosen_expert_weights,
        expert_input_rows,
        expert_norm_gain[None, :],
        queries,
        key_rows,
        value_rows,
        log_decay,
        head_norm_gain,
        output_projection_weight,
        expert_gate_weight,
        expert_up_weight,
        expert_down_weight,
    )


def mapped(mesh, nz, nyc, per_chunk):
    finer = Mesh(mesh.devices.reshape(nz, nyc, NX), EP_TP)
    return jax.shard_map(
        functools.partial(body, nz, nyc, per_chunk),
        mesh=finer,
        in_specs=(
            P(EP, "tp"),
            P(EP, "tp"),
            P(EP, "tp"),
            P(EP, "tp"),
            P("tp"),
            P(EP),
            P(EP, "tp"),
            P("tp", None),
            P("tp", None),
            P(EP, None),
            P(),
            P(EP, None),
            P(EP, None),
            P(EP, None, "tp"),
            P(EP, None, "tp"),
            P(EP, "tp", None),
        ),
        out_specs=(P(EP_TP, None), P(EP, "tp")),
        check_vma=False,
    )


def solution(mesh):
    return mapped(mesh, 8, 8, 2)
```

```python
import functools

import jax
import jax.numpy as jnp
from jax import lax
from jax.experimental import pallas as pl
from jax.experimental.pallas import tpu as pltpu
from jax.sharding import Mesh
from jax.sharding import PartitionSpec as P

F32, BF16 = jnp.float32, jnp.bfloat16
MESH = pl.DeviceIdType.MESH
NX = 4
CAP = 16
BLOCK = 128
LEVELS = (64, 32, 16, 8, 4, 2, 1)
EPS = 1e-06
EP = ("z", "y", "c")
EP_TP = ("z", "y", "c", "tp")


def dot(a, b):
    return jnp.dot(a, b, preferred_element_type=F32)


def dot_nt(a, b):
    return lax.dot_general(a, b, (((1,), (1,)), ((), ())), preferred_element_type=F32)


def dot_tn(a, b):
    return lax.dot_general(a, b, (((0,), (0,)), ((), ())), preferred_element_type=F32)


def iota(shape, dim):
    return lax.broadcasted_iota(jnp.int32, shape, dim)


def one_where(mask):
    return jnp.where(mask, 1.0, 0.0)


CHUNKS = {
    1: ((0,),),
    2: ((0,), (1,)),
    8: ((6,), (2,), (5,), (3,), (4,), (7,), (1,), (0,)),
}
QUARTERS = {1: (2,), 2: (4, 1), 8: (1, 1, 1, 1, 1, 1, 1, 4)}
PLACE = (0, 2, 1, 3)
STEPS = (
    "ds1", "fy0", "ds6", "ds2", "fx0", "wr0", "fy1", "ds3", "ds5", "wy1", "fy6", "fx1", "ds4", "fy2", "wy2", "rl0",
    "fx6", "gla0", "ds7", "wy3", "fx2", "rl1", "fy5", "rl6", "fy3", "gla1", "gla2", "wz1", "fx5", "fx3", "ex0",
    "gla3", "rl5", "sy0", "rl2", "fy4", "rl3", "ap6", "fy7", "fx4", "ex3", "ex1", "ex2", "wz2", "wz3", "sz0", "rl4",
    "ap3", "gy6", "ap5", "ex5", "ex4", "gz6", "gy3", "ap2", "ex6", "gy5", "gz3", "ap4", "gz5", "ap7", "gy2", "ex7",
    "ap1", "cb6", "gz2", "gy4", "gy7", "ap0", "gz4", "wc0", "cb3", "gy1", "mx0", "gz7", "gy0", "cb2", "cb5", "gz1",
    "gz0", "me0", "cb4", "cb0", "cb7", "cb1",
)


def program_of(count):
    if count == 8:
        steps = STEPS
    else:
        order = sum(CHUNKS[count], ())
        quarters = QUARTERS[count]
        steps = [f"ds{d}" for d in order if d] + [f"fy{d}" for d in order]
        steps += ["wr0", "gla0", "gla1", "sy0", "wy1", "wy2", "wy3", "wz1", "wz2", "wz3", "wc0"]
        steps += [f"fx{d}" for d in order if quarters[d] < 4] + [f"rl{d}" for d in order if quarters[d] < 2]
        steps += ["sz0", "mx0"] + [f"ex{c}" for c in range(len(CHUNKS[count]))] + ["me0"]
        for name in ("ap", "gy", "gz", "cb"):
            steps += [f"{name}{d}" for d in order]
    return [(t.rstrip("0123456789"), int(t[len(t.rstrip("0123456789")) :])) for t in steps]


def kernel(
    nz,
    ny,
    nc,
    routes_t,
    chosen_t,
    gain,
    rate,
    position_factor,
    extra_t,
    head_gain,
    rows_hbm,
    queries_hbm,
    keys_hbm,
    values_hbm,
    forget_hbm,
    out_weight_hbm,
    gate_hbm,
    up_hbm,
    down_hbm,
    mix_out,
    moe_out,
    rows,
    queries,
    keys,
    values,
    forget,
    out_weight,
    input_sem,
    mix_held,
    moe_held,
    mixed,
    output_sem,
    gate_w,
    up_w,
    down_w,
    weight_sem,
    zsnd,
    zin,
    xq,
    part,
    pass_a,
    pass_b,
    from_left,
    from_right,
    result,
    yin,
    zret,
    zs,
    zr,
    ys,
    yr,
    xs,
    xr,
    ps,
    pr,
    y2s,
    y2r,
    z2s,
    z2r,
    sums,
    local_out,
    decayed_q,
    state,
    total,
    normed,
    sy,
    tz,
    sz,
    incoming,
    before,
    sys_,
    syr,
    szs,
    szr,
    normed_all,
    ms,
    mr,
    ws,
    wr,
):
    z, y, c, x = (lax.axis_index(a) for a in EP_TP)
    nyc = ny * nc
    yc = y * nc + c
    right, left, opposite = lax.rem(x + 1, NX), lax.rem(x + NX - 1, NX), lax.rem(x + 2, NX)

    def at_yc(index):
        return {"y": lax.div(index, nc), "c": lax.rem(index, nc)}

    order = sum(CHUNKS[nz], ())
    quarters = [QUARTERS[nz][d] for d in order]
    zrows = nyc * CAP
    half = zrows // 2
    quarter = rows.shape[1] // NX
    tokens = rows.shape[0]
    length = queries.shape[0]
    blocks = length // BLOCK

    def remote(src, dst, send, recv, device):
        return pltpu.make_async_remote_copy(
            src_ref=src, dst_ref=dst, send_sem=send, recv_sem=recv, device_id=device, device_id_type=MESH
        )

    def arrived(ref, sem):
        pltpu.make_async_copy(ref, ref, sem).wait()

    def times(value, unit):
        return pl.multiple_of(value * unit, unit)

    def columns(r):
        return pl.ds(PLACE[r] * quarter, quarter)

    def leading(k):
        return pl.ds(0, quarters[k] * quarter)

    barrier = pltpu.get_barrier_semaphore()
    pl.semaphore_signal(barrier, inc=1, device_id={"tp": right}, device_id_type=MESH)
    pl.semaphore_signal(barrier, inc=1, device_id={"tp": left}, device_id_type=MESH)

    pl.semaphore_signal(barrier, inc=1, device_id={"tp": opposite}, device_id_type=MESH)

    def greet_z(t, carry):
        pl.semaphore_signal(barrier, inc=1, device_id={"z": lax.rem(z + t, nz)}, device_id_type=MESH)
        return carry

    def greet_y(t, carry):
        pl.semaphore_signal(barrier, inc=1, device_id=at_yc(lax.rem(yc + t, nyc)), device_id_type=MESH)
        return carry

    lax.fori_loop(1, nz, greet_z, 0)
    lax.fori_loop(1, nyc, greet_y, 0)

    inputs = [
        pltpu.make_async_copy(a, b, input_sem.at[n])
        for n, (a, b) in enumerate(
            (
                (rows_hbm, rows),
                (forget_hbm, forget),
                (queries_hbm, queries),
                (keys_hbm, keys),
                (values_hbm, values),
                (out_weight_hbm, out_weight.at[0]),
            )
        )
    ]
    for load in inputs:
        load.start()
    loads = []
    for r in range(NX):
        back = times(lax.rem(x + NX - r, NX), quarter)
        ahead = times(lax.rem(x + r, NX), quarter)
        loads += [
            pltpu.make_async_copy(gate_hbm.at[0, pl.ds(back, quarter), :], gate_w.at[columns(r), :], weight_sem.at[0]),
            pltpu.make_async_copy(up_hbm.at[0, pl.ds(back, quarter), :], up_w.at[columns(r), :], weight_sem.at[1]),
            pltpu.make_async_copy(down_hbm.at[0, :, pl.ds(ahead, quarter)], down_w.at[:, columns(r)], weight_sem.at[2]),
        ]
    for load in loads:
        load.start()

    experts = nz * nyc
    first_t, second_t = routes_t[0:1, :], routes_t[1:2, :]
    marks = [one_where(iota((experts, tokens), 0) == e) for e in (first_t, second_t)]
    upper = one_where(iota((tokens, tokens), 0) < iota((tokens, tokens), 1)).astype(BF16)
    ranks = [dot(m.astype(BF16), upper) for m in marks]
    ranks[1] = ranks[1] + jnp.sum(marks[0], axis=1, keepdims=True)
    slots_t = [
        e.astype(F32) * CAP + jnp.sum(m * r, axis=0, keepdims=True)
        for e, m, r in zip((first_t, second_t), marks, ranks)
    ]

    inputs[0].wait()
    squares = rows[...].astype(F32)
    scale = lax.rsqrt(jnp.mean(squares * squares, axis=1, keepdims=True) + EPS)

    def moe_normed(r):
        here = pl.ds(times(lax.rem(x + NX - r, NX), quarter), quarter)
        return (rows[:, here].astype(F32) * scale * gain[:, here]).astype(BF16)

    own = moe_normed(0)

    pl.semaphore_wait(barrier, 3 + (nz - 1) + (nyc - 1))

    def dispatch(d):
        k = order.index(d)
        slot = (iota((zrows, tokens), 0) + lax.rem(z + d, nz) * zrows).astype(F32)
        chooser = one_where((slot == slots_t[0]) | (slot == slots_t[1])).astype(BF16)
        for r in (0, 2, 1, 3):
            if PLACE[r] < quarters[k]:
                zsnd[k, :, columns(r)] = dot(chooser, moe_normed(r) if r else own).astype(BF16)

    def send_z(k):
        target = {"z": lax.rem(z + order[k], nz)}
        remote(zsnd.at[k, :, leading(k)], zin.at[k, :, leading(k)], zs.at[quarters[k] // 2], zr.at[k], target).start()

    def forward_y(k):
        source = zin if order[k] else zsnd
        if order[k]:
            arrived(zin.at[k, :, leading(k)], zr.at[k])
        there = pl.ds(pl.multiple_of(k * zrows + yc * CAP, CAP), CAP)

        def send(t, carry):
            to = lax.rem(yc + t, nyc)
            remote(
                source.at[k, pl.ds(times(to, CAP), CAP), leading(k)],
                xq.at[there, leading(k)],
                ys.at[quarters[k] // 2],
                yr.at[k],
                at_yc(to),
            ).start()
            return carry

        lax.fori_loop(1, nyc, send, 0)
        xq[there, leading(k)] = source[k, pl.ds(times(yc, CAP), CAP), leading(k)]

    def forward_x(k):
        mine = xq.at[pl.ds(k * zrows, zrows), columns(0)]
        arrived(xq.at[pl.ds(k * zrows, zrows - CAP), leading(k)], yr.at[k])
        remote(mine, xq.at[pl.ds(k * zrows, zrows), columns(1)], xs.at[0], xr.at[0, k], {"tp": right}).start()
        remote(mine, xq.at[pl.ds(k * zrows, zrows), columns(3)], xs.at[1], xr.at[1, k], {"tp": left}).start()

    def relay(k):
        a, b = pl.ds(k * zrows, half), pl.ds(k * zrows + half, half)
        arrived(xq.at[pl.ds(k * zrows, zrows), columns(1)], xr.at[0, k])
        remote(xq.at[a, columns(1)], xq.at[a, columns(2)], xs.at[2], xr.at[2, k], {"tp": right}).start()
        arrived(xq.at[pl.ds(k * zrows, zrows), columns(3)], xr.at[1, k])
        remote(xq.at[b, columns(3)], xq.at[b, columns(2)], xs.at[3], xr.at[3, k], {"tp": left}).start()

    started = []

    def expert(c):
        first = order.index(CHUNKS[nz][c][0])
        members = range(first, first + len(CHUNKS[nz][c]))
        for k in members:
            if quarters[k] == 4:
                arrived(xq.at[pl.ds(k * zrows, zrows - CAP), :], yr.at[k])
            elif quarters[k] == 2:
                arrived(xq.at[pl.ds(k * zrows, zrows), columns(1)], xr.at[0, k])
                arrived(xq.at[pl.ds(k * zrows, zrows), columns(3)], xr.at[1, k])
            else:
                arrived(xq.at[pl.ds(k * zrows, half), columns(2)], xr.at[2, k])
                arrived(xq.at[pl.ds(k * zrows + half, half), columns(2)], xr.at[3, k])
        if not started:
            started.append(c)
            for n, weight in enumerate((gate_w, up_w, down_w)):
                arrived(weight, weight_sem.at[n])
        here = pl.ds(first * zrows, len(members) * zrows)
        gate = dot(xq[here, :], gate_w[...])
        up = dot(xq[here, :], up_w[...])
        hidden = (jax.nn.silu(gate) * up).astype(BF16)
        part[here, :] = dot(hidden, down_w[...]).astype(BF16)
        for k in members:
            a, b = pl.ds(k * zrows, half), pl.ds(k * zrows + half, half)
            remote(part.at[a, columns(2)], pass_a.at[k], ps.at[0], pr.at[0, k], {"tp": right}).start()
            remote(part.at[b, columns(2)], pass_b.at[k], ps.at[1], pr.at[1, k], {"tp": left}).start()

    def add_pass(k):
        here = pl.ds(k * zrows, zrows)
        a, b = pl.ds(k * zrows, half), pl.ds(k * zrows + half, half)
        arrived(pass_a.at[k], pr.at[0, k])
        part[a, columns(1)] = (part[a, columns(1)].astype(F32) + pass_a[k].astype(F32)).astype(BF16)
        remote(part.at[here, columns(1)], from_left.at[here], ps.at[2], pr.at[2, k], {"tp": right}).start()
        arrived(pass_b.at[k], pr.at[1, k])
        part[b, columns(3)] = (part[b, columns(3)].astype(F32) + pass_b[k].astype(F32)).astype(BF16)
        remote(part.at[here, columns(3)], from_right.at[here], ps.at[3], pr.at[3, k], {"tp": left}).start()

    def give_back_y(k):
        here = pl.ds(k * zrows, zrows)
        arrived(from_left.at[here], pr.at[2, k])
        arrived(from_right.at[here], pr.at[3, k])
        result[here, :] = (
            part[here, columns(0)].astype(F32) + from_left[here, :].astype(F32) + from_right[here, :].astype(F32)
        ).astype(BF16)

        def send(t, carry):
            to = lax.rem(yc + t, nyc)
            remote(
                result.at[pl.ds(pl.multiple_of(k * zrows + to * CAP, CAP), CAP), :],
                yin.at[k, pl.ds(times(yc, CAP), CAP), :],
                y2s,
                y2r.at[k],
                at_yc(to),
            ).start()
            return carry

        lax.fori_loop(1, nyc, send, 0)
        yin[k, pl.ds(times(yc, CAP), CAP), :] = result[pl.ds(pl.multiple_of(k * zrows + yc * CAP, CAP), CAP), :]

    def give_back_z(k):
        arrived(yin.at[k, pl.ds(0, zrows - CAP), :], y2r.at[k])
        if order[k]:
            to = lax.rem(z + nz - order[k], nz)
            remote(yin.at[k], zret.at[k], z2s, z2r.at[k], {"z": to}).start()

    combined = []

    def combine(k):
        base = lax.rem(z + order[k], nz) * zrows
        slot = (iota((zrows, tokens), 0) + base).astype(F32)
        weight = jnp.where(slot == slots_t[0], chosen_t[0:1, :], 0.0) + jnp.where(slot == slots_t[1], chosen_t[1:2, :], 0.0)
        high = weight.astype(BF16)
        low = (weight - high.astype(F32)).astype(BF16)
        if order[k]:
            arrived(zret.at[k], z2r.at[k])
        returned = zret[k] if order[k] else yin[k]
        fresh = dot_tn(high, returned) + dot_tn(low, returned)
        mixed[...] = mixed[...] + fresh if combined else fresh
        combined.append(k)

    def prepare_sums():
        i, j = iota((BLOCK, BLOCK), 0), iota((BLOCK, BLOCK), 1)
        for level, h in enumerate(LEVELS):
            edge = (i & ~(2 * h - 1)) + h
            after = (j >= edge) & (j <= i)
            ahead = (j > i) & (j < edge)
            m = one_where(after | ahead).astype(BF16)
            sums[pl.ds(level * BLOCK, BLOCK), pl.ds(0, BLOCK)] = m
            sums[pl.ds(level * BLOCK, BLOCK), pl.ds(BLOCK, BLOCK)] = m
        for level, m in ((len(LEVELS), j <= i), (len(LEVELS) + 1, j > i)):
            m = one_where(m).astype(BF16)
            sums[pl.ds(level * BLOCK, BLOCK), pl.ds(0, BLOCK)] = m
            sums[pl.ds(level * BLOCK, BLOCK), pl.ds(BLOCK, BLOCK)] = m

    first_head = iota((BLOCK, BLOCK), 1) < BLOCK // 2

    def by_head(value):
        return jnp.concatenate([jnp.where(first_head, value, 0.0), jnp.where(first_head, 0.0, value)], axis=0).astype(BF16)

    def gla_block(b):
        if b == 0:
            for load in inputs[1:5]:
                load.wait()
        r = pl.ds(b * BLOCK, BLOCK)
        factors = jnp.concatenate([position_factor[:, r], extra_t[:, r], jnp.zeros((5, BLOCK), F32)], axis=0).T
        f = forget[r, :].astype(F32)
        g = (jnp.minimum(f, 0.0) - jnp.log1p(jnp.exp(-jnp.abs(f)))) * rate[...] * factors[:, 0:1]
        g = g + jnp.where(first_head, factors[:, 1:2], factors[:, 2:3])
        high = g.astype(BF16)
        low = (g - high.astype(F32)).astype(BF16)
        e = jnp.exp(dot(sums[...], jnp.concatenate([high, low], axis=0)))
        q, k = queries[r, :].astype(F32), keys[r, :].astype(F32)
        i, j = iota((BLOCK, 2 * BLOCK), 0), iota((BLOCK, 2 * BLOCK), 1) & (BLOCK - 1)
        apart = i ^ j
        scores = None
        for level, h in enumerate(LEVELS):
            factor = e[level * BLOCK : (level + 1) * BLOCK]
            s = dot_nt((q * factor).astype(BF16), by_head(k * factor))
            scores = s if scores is None else jnp.where(apart < 2 * h, s, scores)
        scores = jnp.where(apart < 1, dot_nt(queries[r, :], by_head(k)), scores)
        scores = jnp.where(i >= j, scores, 0.0).astype(BF16)
        n = len(LEVELS)
        from_start = e[n * BLOCK : (n + 1) * BLOCK]
        to_end = e[(n + 1) * BLOCK : (n + 2) * BLOCK]
        qg = q * from_start
        outs = [
            dot(scores[:, h * BLOCK : (h + 1) * BLOCK], values[r, pl.ds(h * BLOCK, BLOCK)]) for h in range(2)
        ]
        if b:
            carried = dot_nt(by_head(qg), state[...].astype(BF16))
            outs = [o + carried[h * BLOCK : (h + 1) * BLOCK] for h, o in enumerate(outs)]
            decayed_q[r, :] = (qg * total[...]).astype(BF16)
        else:
            decayed_q[r, :] = qg.astype(BF16)
        for h in range(2):
            local_out[r, pl.ds(h * BLOCK, BLOCK)] = outs[h]
        grown = dot_tn(values[r, :], (k * to_end).astype(BF16))
        fresh = jnp.where(first_head, grown[0:BLOCK], grown[BLOCK : 2 * BLOCK])
        through = from_start[BLOCK - 1 : BLOCK, :]
        if b:
            state[...] = state[...] * through + fresh
            total[...] = total[...] * through
        else:
            state[...] = fresh
            total[...] = through

    def packed(s, d):
        high = d.astype(BF16).astype(F32)
        row = iota((16, BLOCK), 0)
        tail = jnp.where(row == 0, high, jnp.where(row == 1, d - high, 0.0))
        return s.astype(BF16), tail.astype(BF16)

    def opened(ref, at):
        tail = ref[at, pl.ds(BLOCK, 16), :].astype(F32)
        return ref[at, pl.ds(0, BLOCK), :].astype(F32), tail[0:1] + tail[1:2]

    def states_y():
        s, tail = packed(state[...], total[...])
        tz[1, pl.ds(0, BLOCK), :] = s
        tz[1, pl.ds(BLOCK, 16), :] = tail

        def send(t, carry):
            to = lax.rem(yc + t, nyc)
            remote(tz.at[1], sy.at[yc], sys_, syr, at_yc(to)).start()
            return carry

        lax.fori_loop(1, nyc, send, 0)
        sy[yc, pl.ds(0, BLOCK), :] = s
        sy[yc, pl.ds(BLOCK, 16), :] = tail

    def states_z():
        arrived(sy.at[pl.ds(0, nyc - 1)], syr)
        run_s, run_d = jnp.zeros((BLOCK, BLOCK), F32), jnp.ones((1, BLOCK), F32)
        before[pl.ds(0, BLOCK), :] = run_s
        before[pl.ds(BLOCK, 8), :] = jnp.broadcast_to(run_d, (8, BLOCK))
        for s in range(nyc):
            new_s, new_d = opened(sy, s)
            run_s, run_d = run_s * new_d + new_s, run_d * new_d

            @pl.when(s < yc)
            def _(run_s=run_s, run_d=run_d):
                before[pl.ds(0, BLOCK), :] = run_s
                before[pl.ds(BLOCK, 8), :] = jnp.broadcast_to(run_d, (8, BLOCK))

        s, tail = packed(run_s, run_d)
        tz[0, pl.ds(0, BLOCK), :] = s
        tz[0, pl.ds(BLOCK, 16), :] = tail
        for d in range(1, nz):

            @pl.when(z + d < nz)
            def _(d=d):
                remote(tz.at[0], sz.at[z], szs.at[d], szr.at[z], {"z": z + d}).start()

    def states_in():
        incoming[...] = jnp.zeros((BLOCK, BLOCK), F32)
        for s in range(nz - 1):

            @pl.when(s < z)
            def _(s=s):
                arrived(sz.at[s], szr.at[s])
                new_s, new_d = opened(sz, s)
                incoming[...] = incoming[...] * new_d + new_s

        incoming[...] = incoming[...] * before[pl.ds(BLOCK, 8), :][0:1] + before[pl.ds(0, BLOCK), :]

    mrows = length // NX
    width_of_group = 2 * BLOCK

    def mix():
        s = incoming[...].astype(BF16)
        for b in range(blocks):
            r = pl.ds(b * BLOCK, BLOCK)
            carried = dot_nt(by_head(decayed_q[r, :].astype(F32)), s)
            for h in range(2):
                c = pl.ds(h * BLOCK, BLOCK)
                o = local_out[r, c] + carried[h * BLOCK : (h + 1) * BLOCK]
                o = o * lax.rsqrt(jnp.mean(o * o, axis=1, keepdims=True) + EPS) * head_gain[h : h + 1, :]
                normed[r, c] = o.astype(BF16)
        normed_all[:, 0:width_of_group] = normed[pl.ds(times(x, mrows), mrows), :]
        for r, to in ((1, right), (2, opposite), (3, left)):
            remote(
                normed.at[pl.ds(times(to, mrows), mrows), :],
                normed_all.at[:, pl.ds(r * width_of_group, width_of_group)],
                ms,
                mr.at[r],
                {"tp": to},
            ).start()

    piece = out_weight.shape[1] // nyc
    phalf = piece // 2
    above, below = lax.rem(y + 1, ny), lax.rem(y + ny - 1, ny)

    def piece_of(which, start, size):
        return pl.ds(pl.multiple_of((c * ny + which) * piece + start, 16), size)

    def weights_x():
        inputs[5].wait()
        here = piece_of(y, 0, piece)
        remote(out_weight.at[0, here], out_weight.at[1, here], ws, wr.at[0], {"tp": right}).start()
        remote(out_weight.at[0, here], out_weight.at[3, here], ws, wr.at[1], {"tp": left}).start()

    def weights_x_relay():
        here, a, b = piece_of(y, 0, piece), piece_of(y, 0, phalf), piece_of(y, phalf, phalf)
        arrived(out_weight.at[1, here], wr.at[0])
        remote(out_weight.at[1, a], out_weight.at[2, a], ws, wr.at[2], {"tp": right}).start()
        arrived(out_weight.at[3, here], wr.at[1])
        remote(out_weight.at[3, b], out_weight.at[2, b], ws, wr.at[3], {"tp": left}).start()

    others = pl.ds(1, NX - 1)

    def weights_y(r):
        here, a, b = piece_of(y, 0, piece), piece_of(y, 0, phalf), piece_of(y, phalf, phalf)
        if r == 2:
            arrived(out_weight.at[2, a], wr.at[2])
            arrived(out_weight.at[2, b], wr.at[3])
        if ny > 1:
            mine = out_weight.at[r, here]
            remote(mine, mine, ws, wr.at[4 * r], {"y": above}).start()
            remote(mine, mine, ws, wr.at[4 * r + 1], {"y": below}).start()

    def weights_y_relay(r):
        if ny > 1:
            arrived(out_weight.at[r, piece_of(below, 0, piece)], wr.at[4 * r])
            a = out_weight.at[r, piece_of(below, 0, phalf)]
            remote(a, a, ws, wr.at[4 * r + 2], {"y": above}).start()
            arrived(out_weight.at[r, piece_of(above, 0, piece)], wr.at[4 * r + 1])
            b = out_weight.at[r, piece_of(above, phalf, phalf)]
            remote(b, b, ws, wr.at[4 * r + 3], {"y": below}).start()

    def column_of(which):
        return out_weight.at[others, pl.ds(times(which * ny, piece), ny * piece)]

    def weights_c():
        if ny > 1:
            far = lax.rem(y + 2, ny)
            for r in range(1, NX):
                arrived(out_weight.at[r, piece_of(far, 0, phalf)], wr.at[4 * r + 2])
                arrived(out_weight.at[r, piece_of(far, phalf, phalf)], wr.at[4 * r + 3])
        if nc > 1:
            remote(column_of(c), column_of(c), ws, wr.at[4 * NX], {"c": 1 - c}).start()

    def mix_end():
        if nc > 1:
            arrived(column_of(1 - c), wr.at[4 * NX])
        for r in range(1, NX):
            arrived(normed_all.at[:, pl.ds(r * width_of_group, width_of_group)], mr.at[r])
        full = out_weight[...].reshape(NX * width_of_group, out_weight.shape[2])
        mix_held[...] = dot(normed_all[...], full).astype(BF16)
        pltpu.make_async_copy(mix_held, mix_out, output_sem.at[0]).start()

    def at(work):
        return lambda d: work(order.index(d))

    def alone(*works):
        def run(index):
            for work in works:
                work()

        return run

    does = {
        "ds": at(send_z),
        "fy": at(forward_y),
        "fx": at(forward_x),
        "rl": at(relay),
        "ex": expert,
        "ap": at(add_pass),
        "gy": at(give_back_y),
        "gz": at(give_back_z),
        "cb": at(combine),
        "gla": gla_block,
        "sy": alone(states_y),
        "sz": alone(states_z),
        "mx": alone(states_in, mix),
        "me": alone(mix_end),
        "wr": alone(weights_x_relay),
        "wy": weights_y,
        "wz": weights_y_relay,
        "wc": alone(weights_c),
    }
    weights_x()
    for d in sorted(order, key=lambda d: min(d, nz - d)):
        dispatch(d)
    for name, index in program_of(nz):
        if (name, index) == ("gla", 0):
            prepare_sums()
        does[name](index)
    moe_held[...] = mixed[...].astype(BF16)
    pltpu.make_async_copy(moe_held, moe_out, output_sem.at[1]).start()

    for q in sorted(set(quarters)):
        across = pl.ds(0, q * quarter)
        forwarded = quarters.count(q)
        sent = forwarded - (quarters[order.index(0)] == q)
        arrived(xq.at[pl.ds(0, forwarded * (zrows - CAP)), across], ys.at[q // 2])
        if sent:
            arrived(xq.at[pl.ds(0, sent * zrows), across], zs.at[q // 2])
    gathered, relayed = sum(q < 4 for q in quarters), sum(q < 2 for q in quarters)
    for side in range(2):
        if gathered:
            arrived(xq.at[pl.ds(0, gathered * zrows), columns(0)], xs.at[side])
        if relayed:
            arrived(xq.at[pl.ds(0, relayed * half), columns(0)], xs.at[2 + side])
        arrived(xq.at[pl.ds(0, nz * half), columns(0)], ps.at[side])
        arrived(xq.at[pl.ds(0, nz * zrows), columns(0)], ps.at[2 + side])
    arrived(xq.at[pl.ds(0, nz * (zrows - CAP)), columns(0)], y2s)
    if nz > 1:
        arrived(xq.at[pl.ds(0, (nz - 1) * zrows), columns(0)], z2s)
    arrived(sy.at[pl.ds(0, nyc - 1)], sys_)
    for d in range(1, nz):

        @pl.when(z + d < nz)
        def _(d=d):
            arrived(tz.at[0], szs.at[d])

    arrived(normed_all.at[:, pl.ds(0, (NX - 1) * width_of_group)], ms)
    sent = 2 * (piece + phalf) * (NX if ny > 1 else 1) + ((NX - 1) * ny * piece if nc > 1 else 0)
    arrived(out_weight.at[pl.ds(0, sent // out_weight.shape[1])], ws)
    pltpu.make_async_copy(mix_held, mix_out, output_sem.at[0]).wait()
    pltpu.make_async_copy(moe_held, moe_out, output_sem.at[1]).wait()


def body(
    nz,
    ny,
    nc,
    queries,
    key_rows,
    value_rows,
    forget_gate_input,
    channel_decay_rate,
    position_decay_factor,
    extra_log_decay,
    head_norm_gain,
    output_projection_weight,
    expert_input_rows,
    expert_norm_gain,
    routes,
    chosen_expert_weights,
    expert_gate_weight,
    expert_up_weight,
    expert_down_weight,
):
    length, channels = queries.shape
    tokens, width = expert_input_rows.shape
    hidden = expert_gate_weight.shape[2]
    quarter = width // NX
    nyc = ny * nc
    zrows = nyc * CAP
    dma, vmem = pltpu.SemaphoreType.DMA, pltpu.VMEM
    mrows = length // NX
    outs = pl.pallas_call(
        functools.partial(kernel, nz, ny, nc),
        out_shape=(
            jax.ShapeDtypeStruct((mrows, width), BF16),
            jax.ShapeDtypeStruct((tokens, quarter), BF16),
        ),
        in_specs=[pl.BlockSpec(memory_space=vmem)] * 7 + [pl.BlockSpec(memory_space=pl.ANY)] * 9,
        out_specs=(pl.BlockSpec(memory_space=pl.ANY), pl.BlockSpec(memory_space=pl.ANY)),
        scratch_shapes=[
            vmem((tokens, width), BF16),
            vmem((length, channels), BF16),
            vmem((length, channels), BF16),
            vmem((length, value_rows.shape[1]), BF16),
            vmem((length, channels), BF16),
            vmem((NX, *output_projection_weight.shape), BF16),
            dma((6,)),
            vmem((mrows, width), BF16),
            vmem((tokens, quarter), BF16),
            vmem((tokens, quarter), F32),
            dma((2,)),
            vmem((width, hidden), BF16),
            vmem((width, hidden), BF16),
            vmem((hidden, width), BF16),
            dma((3,)),
            vmem((nz, zrows, width), BF16),
            vmem((nz, zrows, width), BF16),
            vmem((nz * zrows, width), BF16),
            vmem((nz * zrows, width), BF16),
            vmem((nz, zrows // 2, quarter), BF16),
            vmem((nz, zrows // 2, quarter), BF16),
            vmem((nz * zrows, quarter), BF16),
            vmem((nz * zrows, quarter), BF16),
            vmem((nz * zrows, quarter), BF16),
            vmem((nz, zrows, quarter), BF16),
            vmem((nz, zrows, quarter), BF16),
            dma((3,)),
            dma((nz,)),
            dma((3,)),
            dma((nz,)),
            dma((4,)),
            dma((4, nz)),
            dma((4,)),
            dma((4, nz)),
            dma(()),
            dma((nz,)),
            dma(()),
            dma((nz,)),
            vmem(((len(LEVELS) + 2) * BLOCK, 2 * BLOCK), BF16),
            vmem((length, 2 * BLOCK), F32),
            vmem((length, BLOCK), BF16),
            vmem((BLOCK, BLOCK), F32),
            vmem((1, BLOCK), F32),
            vmem((length, 2 * BLOCK), BF16),
            vmem((nyc, BLOCK + 16, BLOCK), BF16),
            vmem((2, BLOCK + 16, BLOCK), BF16),
            vmem((nz, BLOCK + 16, BLOCK), BF16),
            vmem((BLOCK, BLOCK), F32),
            vmem((BLOCK + 8, BLOCK), F32),
            dma(()),
            dma(()),
            dma((nz,)),
            dma((nz,)),
            vmem((mrows, NX * value_rows.shape[1]), BF16),
            dma(()),
            dma((NX,)),
            dma(()),
            dma((4 * NX + 1,)),
        ],
        compiler_params=pltpu.CompilerParams(
            collective_id=0, has_side_effects=True, vmem_limit_bytes=60 * 1024 * 1024
        ),
        name="mixer_and_experts",
    )(
        routes.T,
        chosen_expert_weights.T,
        expert_norm_gain[None, :],
        channel_decay_rate[None, :],
        position_decay_factor[None, :],
        extra_log_decay.T,
        head_norm_gain,
        expert_input_rows,
        queries,
        key_rows,
        value_rows,
        forget_gate_input,
        output_projection_weight,
        expert_gate_weight,
        expert_up_weight,
        expert_down_weight,
    )
    return pl.pallas_call(
        handed_over,
        out_shape=tuple(jax.ShapeDtypeStruct(o.shape, o.dtype) for o in outs),
        in_specs=[pl.BlockSpec(memory_space=vmem)] * 2,
        out_specs=(pl.BlockSpec(memory_space=vmem),) * 2,
        name="handed_over",
    )(*outs)


def handed_over(mix_in, moe_in, mix_out, moe_out):
    mix_out[...] = mix_in[...]
    moe_out[...] = moe_in[...]


def mapped(mesh, nz, ny, nc):
    finer = Mesh(mesh.devices.reshape(nz, ny, nc, NX), EP_TP)
    return jax.shard_map(
        functools.partial(body, nz, ny, nc),
        mesh=finer,
        in_specs=(
            P(EP, "tp"),
            P(EP, "tp"),
            P(EP, "tp"),
            P(EP, "tp"),
            P("tp"),
            P(EP),
            P(EP, "tp"),
            P("tp", None),
            P("tp", None),
            P(EP, None),
            P(),
            P(EP, None),
            P(EP, None),
            P(EP, None, "tp"),
            P(EP, None, "tp"),
            P(EP, "tp", None),
        ),
        out_specs=(P(EP_TP, None), P(EP, "tp")),
        check_vma=False,
    )


def solution(mesh):
    return mapped(mesh, 8, 4, 2)
```

```python
import functools

import jax
import jax.numpy as jnp
from jax import lax
from jax.experimental import pallas as pl
from jax.experimental.pallas import tpu as pltpu
from jax.sharding import Mesh
from jax.sharding import PartitionSpec as P

F32, BF16 = jnp.float32, jnp.bfloat16
MESH = pl.DeviceIdType.MESH
NX = 4
CAP = 16
BLOCK = 128
LEVELS = (64, 32, 16, 8, 4, 2, 1)
EPS = 1e-06
EP = ("z", "y", "c")
EP_TP = ("z", "y", "c", "tp")


def dot(a, b):
    return jnp.dot(a, b, preferred_element_type=F32)


def dot_nt(a, b):
    return lax.dot_general(a, b, (((1,), (1,)), ((), ())), preferred_element_type=F32)


def dot_tn(a, b):
    return lax.dot_general(a, b, (((0,), (0,)), ((), ())), preferred_element_type=F32)


def iota(shape, dim):
    return lax.broadcasted_iota(jnp.int32, shape, dim)


def one_where(mask):
    return jnp.where(mask, 1.0, 0.0)


CHUNKS = {
    1: ((0,),),
    2: ((0,), (1,)),
    8: ((6,), (2,), (5,), (3,), (4,), (7,), (1,), (0,)),
}
QUARTERS = {1: (2,), 2: (4, 1), 8: (1, 1, 1, 1, 1, 1, 1, 4)}
PLACE = (0, 2, 1, 3)
STEPS = (
    "ds1", "fy0", "ds6", "ds2", "fx0", "wr0", "fy1", "ds3", "ds5", "wy1", "fy6", "fx1", "ds4", "fy2", "wy2", "rl0",
    "fx6", "gla0", "ds7", "wy3", "fx2", "rl1", "fy5", "rl6", "fy3", "gla1", "gla2", "wz1", "fx5", "fx3", "ex0",
    "gla3", "rl5", "sy0", "rl2", "fy4", "rl3", "ap6", "fy7", "fx4", "ex3", "ex1", "ex2", "wz2", "wz3", "sz0", "rl4",
    "ap3", "gy6", "ap5", "ex5", "ex4", "gz6", "gy3", "ap2", "ex6", "gy5", "gz3", "ap4", "gz5", "ap7", "gy2", "ex7",
    "ap1", "cb6", "gz2", "gy4", "gy7", "ap0", "gz4", "wc0", "cb3", "gy1", "mx0", "gz7", "gy0", "cb2", "cb5", "gz1",
    "gz0", "me0", "cb4", "cb0", "cb7", "cb1",
)


def program_of(count):
    if count == 8:
        steps = STEPS
    else:
        order = sum(CHUNKS[count], ())
        quarters = QUARTERS[count]
        steps = [f"ds{d}" for d in order if d] + [f"fy{d}" for d in order]
        steps += ["wr0", "gla0", "gla1", "sy0", "wy1", "wy2", "wy3", "wz1", "wz2", "wz3", "wc0"]
        steps += [f"fx{d}" for d in order if quarters[d] < 4] + [f"rl{d}" for d in order if quarters[d] < 2]
        steps += ["sz0", "mx0"] + [f"ex{c}" for c in range(len(CHUNKS[count]))] + ["me0"]
        for name in ("ap", "gy", "gz", "cb"):
            steps += [f"{name}{d}" for d in order]
    return [(t.rstrip("0123456789"), int(t[len(t.rstrip("0123456789")) :])) for t in steps]


def kernel(
    nz,
    ny,
    nc,
    routes_hbm,
    chosen_hbm,
    gain_hbm,
    rate_hbm,
    position_hbm,
    extra_hbm,
    head_gain_hbm,
    rows_hbm,
    queries_hbm,
    keys_hbm,
    values_hbm,
    forget_hbm,
    out_weight_hbm,
    gate_hbm,
    up_hbm,
    down_hbm,
    mix_out,
    moe_out,
    routes_t,
    chosen_t,
    gain,
    rate,
    position_factor,
    extra_t,
    head_gain,
    rows,
    queries,
    keys,
    values,
    forget,
    out_weight,
    small_sem,
    input_sem,
    mix_held,
    moe_held,
    mixed,
    output_sem,
    gate_w,
    up_w,
    down_w,
    weight_sem,
    zsnd,
    zin,
    xq,
    part,
    pass_a,
    pass_b,
    from_left,
    from_right,
    result,
    yin,
    zret,
    zs,
    zr,
    ys,
    yr,
    xs,
    xr,
    ps,
    pr,
    y2s,
    y2r,
    z2s,
    z2r,
    sums,
    local_out,
    decayed_q,
    state,
    total,
    normed,
    sy,
    tz,
    sz,
    incoming,
    before,
    sys_,
    syr,
    szs,
    szr,
    normed_all,
    ms,
    mr,
    ws,
    wr,
):
    z, y, c, x = (lax.axis_index(a) for a in EP_TP)
    nyc = ny * nc
    yc = y * nc + c
    right, left, opposite = lax.rem(x + 1, NX), lax.rem(x + NX - 1, NX), lax.rem(x + 2, NX)

    def at_yc(index):
        return {"y": lax.div(index, nc), "c": lax.rem(index, nc)}

    order = sum(CHUNKS[nz], ())
    quarters = [QUARTERS[nz][d] for d in order]
    zrows = nyc * CAP
    half = zrows // 2
    quarter = rows.shape[1] // NX
    tokens = rows.shape[0]
    length = queries.shape[0]
    blocks = length // BLOCK

    def remote(src, dst, send, recv, device):
        return pltpu.make_async_remote_copy(
            src_ref=src, dst_ref=dst, send_sem=send, recv_sem=recv, device_id=device, device_id_type=MESH
        )

    def arrived(ref, sem):
        pltpu.make_async_copy(ref, ref, sem).wait()

    def times(value, unit):
        return pl.multiple_of(value * unit, unit)

    def columns(r):
        return pl.ds(PLACE[r] * quarter, quarter)

    def leading(k):
        return pl.ds(0, quarters[k] * quarter)

    barrier = pltpu.get_barrier_semaphore()
    pl.semaphore_signal(barrier, inc=1, device_id={"tp": right}, device_id_type=MESH)
    pl.semaphore_signal(barrier, inc=1, device_id={"tp": left}, device_id_type=MESH)

    pl.semaphore_signal(barrier, inc=1, device_id={"tp": opposite}, device_id_type=MESH)

    def greet_z(t, carry):
        pl.semaphore_signal(barrier, inc=1, device_id={"z": lax.rem(z + t, nz)}, device_id_type=MESH)
        return carry

    def greet_y(t, carry):
        pl.semaphore_signal(barrier, inc=1, device_id=at_yc(lax.rem(yc + t, nyc)), device_id_type=MESH)
        return carry

    lax.fori_loop(1, nz, greet_z, 0)
    lax.fori_loop(1, nyc, greet_y, 0)

    small = [
        pltpu.make_async_copy(a, b, small_sem.at[n])
        for n, (a, b) in enumerate(
            (
                (routes_hbm, routes_t),
                (gain_hbm, gain),
                (chosen_hbm, chosen_t),
                (rate_hbm, rate),
                (position_hbm, position_factor),
                (extra_hbm, extra_t),
                (head_gain_hbm, head_gain),
            )
        )
    ]
    inputs = [
        pltpu.make_async_copy(a, b, input_sem.at[n])
        for n, (a, b) in enumerate(
            (
                (rows_hbm, rows),
                (forget_hbm, forget),
                (queries_hbm, queries),
                (keys_hbm, keys),
                (values_hbm, values),
                (out_weight_hbm, out_weight.at[0]),
            )
        )
    ]
    for load in small[:1] + inputs[:1] + small[1:] + inputs[1:]:
        load.start()
    loads = []
    for r in range(NX):
        back = times(lax.rem(x + NX - r, NX), quarter)
        ahead = times(lax.rem(x + r, NX), quarter)
        loads += [
            pltpu.make_async_copy(gate_hbm.at[0, pl.ds(back, quarter), :], gate_w.at[columns(r), :], weight_sem.at[0]),
            pltpu.make_async_copy(up_hbm.at[0, pl.ds(back, quarter), :], up_w.at[columns(r), :], weight_sem.at[1]),
            pltpu.make_async_copy(down_hbm.at[0, :, pl.ds(ahead, quarter)], down_w.at[:, columns(r)], weight_sem.at[2]),
        ]
    for load in loads:
        load.start()

    small[0].wait()
    experts = nz * nyc
    first_t, second_t = routes_t[0:1, :], routes_t[1:2, :]
    marks = [one_where(iota((experts, tokens), 0) == e) for e in (first_t, second_t)]
    upper = one_where(iota((tokens, tokens), 0) < iota((tokens, tokens), 1)).astype(BF16)
    ranks = [dot(m.astype(BF16), upper) for m in marks]
    ranks[1] = ranks[1] + jnp.sum(marks[0], axis=1, keepdims=True)
    slots_t = [
        e.astype(F32) * CAP + jnp.sum(m * r, axis=0, keepdims=True)
        for e, m, r in zip((first_t, second_t), marks, ranks)
    ]

    small[1].wait()
    inputs[0].wait()
    squares = rows[...].astype(F32)
    scale = lax.rsqrt(jnp.mean(squares * squares, axis=1, keepdims=True) + EPS)

    def moe_normed(r):
        here = pl.ds(times(lax.rem(x + NX - r, NX), quarter), quarter)
        return (rows[:, here].astype(F32) * scale * gain[:, here]).astype(BF16)

    own = moe_normed(0)

    def dispatch(d):
        k = order.index(d)
        slot = (iota((zrows, tokens), 0) + lax.rem(z + d, nz) * zrows).astype(F32)
        chooser = one_where((slot == slots_t[0]) | (slot == slots_t[1])).astype(BF16)
        for r in (0, 2, 1, 3):
            if PLACE[r] < quarters[k]:
                zsnd[k, :, columns(r)] = dot(chooser, moe_normed(r) if r else own).astype(BF16)

    def send_z(k):
        target = {"z": lax.rem(z + order[k], nz)}
        remote(zsnd.at[k, :, leading(k)], zin.at[k, :, leading(k)], zs.at[quarters[k] // 2], zr.at[k], target).start()

    def forward_y(k):
        source = zin if order[k] else zsnd
        if order[k]:
            arrived(zin.at[k, :, leading(k)], zr.at[k])
        there = pl.ds(pl.multiple_of(k * zrows + yc * CAP, CAP), CAP)

        def send(t, carry):
            to = lax.rem(yc + t, nyc)
            remote(
                source.at[k, pl.ds(times(to, CAP), CAP), leading(k)],
                xq.at[there, leading(k)],
                ys.at[quarters[k] // 2],
                yr.at[k],
                at_yc(to),
            ).start()
            return carry

        lax.fori_loop(1, nyc, send, 0)
        xq[there, leading(k)] = source[k, pl.ds(times(yc, CAP), CAP), leading(k)]

    def forward_x(k):
        mine = xq.at[pl.ds(k * zrows, zrows), columns(0)]
        arrived(xq.at[pl.ds(k * zrows, zrows - CAP), leading(k)], yr.at[k])
        remote(mine, xq.at[pl.ds(k * zrows, zrows), columns(1)], xs.at[0], xr.at[0, k], {"tp": right}).start()
        remote(mine, xq.at[pl.ds(k * zrows, zrows), columns(3)], xs.at[1], xr.at[1, k], {"tp": left}).start()

    def relay(k):
        a, b = pl.ds(k * zrows, half), pl.ds(k * zrows + half, half)
        arrived(xq.at[pl.ds(k * zrows, zrows), columns(1)], xr.at[0, k])
        remote(xq.at[a, columns(1)], xq.at[a, columns(2)], xs.at[2], xr.at[2, k], {"tp": right}).start()
        arrived(xq.at[pl.ds(k * zrows, zrows), columns(3)], xr.at[1, k])
        remote(xq.at[b, columns(3)], xq.at[b, columns(2)], xs.at[3], xr.at[3, k], {"tp": left}).start()

    started = []

    def expert(c):
        first = order.index(CHUNKS[nz][c][0])
        members = range(first, first + len(CHUNKS[nz][c]))
        for k in members:
            if quarters[k] == 4:
                arrived(xq.at[pl.ds(k * zrows, zrows - CAP), :], yr.at[k])
            elif quarters[k] == 2:
                arrived(xq.at[pl.ds(k * zrows, zrows), columns(1)], xr.at[0, k])
                arrived(xq.at[pl.ds(k * zrows, zrows), columns(3)], xr.at[1, k])
            else:
                arrived(xq.at[pl.ds(k * zrows, half), columns(2)], xr.at[2, k])
                arrived(xq.at[pl.ds(k * zrows + half, half), columns(2)], xr.at[3, k])
        if not started:
            started.append(c)
            for n, weight in enumerate((gate_w, up_w, down_w)):
                arrived(weight, weight_sem.at[n])
        here = pl.ds(first * zrows, len(members) * zrows)
        gate = dot(xq[here, :], gate_w[...])
        up = dot(xq[here, :], up_w[...])
        hidden = (jax.nn.silu(gate) * up).astype(BF16)
        part[here, :] = dot(hidden, down_w[...]).astype(BF16)
        for k in members:
            a, b = pl.ds(k * zrows, half), pl.ds(k * zrows + half, half)
            remote(part.at[a, columns(2)], pass_a.at[k], ps.at[0], pr.at[0, k], {"tp": right}).start()
            remote(part.at[b, columns(2)], pass_b.at[k], ps.at[1], pr.at[1, k], {"tp": left}).start()

    def add_pass(k):
        here = pl.ds(k * zrows, zrows)
        a, b = pl.ds(k * zrows, half), pl.ds(k * zrows + half, half)
        arrived(pass_a.at[k], pr.at[0, k])
        part[a, columns(1)] = (part[a, columns(1)].astype(F32) + pass_a[k].astype(F32)).astype(BF16)
        remote(part.at[here, columns(1)], from_left.at[here], ps.at[2], pr.at[2, k], {"tp": right}).start()
        arrived(pass_b.at[k], pr.at[1, k])
        part[b, columns(3)] = (part[b, columns(3)].astype(F32) + pass_b[k].astype(F32)).astype(BF16)
        remote(part.at[here, columns(3)], from_right.at[here], ps.at[3], pr.at[3, k], {"tp": left}).start()

    def give_back_y(k):
        here = pl.ds(k * zrows, zrows)
        arrived(from_left.at[here], pr.at[2, k])
        arrived(from_right.at[here], pr.at[3, k])
        result[here, :] = (
            part[here, columns(0)].astype(F32) + from_left[here, :].astype(F32) + from_right[here, :].astype(F32)
        ).astype(BF16)

        def send(t, carry):
            to = lax.rem(yc + t, nyc)
            remote(
                result.at[pl.ds(pl.multiple_of(k * zrows + to * CAP, CAP), CAP), :],
                yin.at[k, pl.ds(times(yc, CAP), CAP), :],
                y2s,
                y2r.at[k],
                at_yc(to),
            ).start()
            return carry

        lax.fori_loop(1, nyc, send, 0)
        yin[k, pl.ds(times(yc, CAP), CAP), :] = result[pl.ds(pl.multiple_of(k * zrows + yc * CAP, CAP), CAP), :]

    def give_back_z(k):
        arrived(yin.at[k, pl.ds(0, zrows - CAP), :], y2r.at[k])
        if order[k]:
            to = lax.rem(z + nz - order[k], nz)
            remote(yin.at[k], zret.at[k], z2s, z2r.at[k], {"z": to}).start()

    combined = []

    def combine(k):
        base = lax.rem(z + order[k], nz) * zrows
        slot = (iota((zrows, tokens), 0) + base).astype(F32)
        weight = jnp.where(slot == slots_t[0], chosen_t[0:1, :], 0.0) + jnp.where(slot == slots_t[1], chosen_t[1:2, :], 0.0)
        high = weight.astype(BF16)
        low = (weight - high.astype(F32)).astype(BF16)
        if order[k]:
            arrived(zret.at[k], z2r.at[k])
        returned = zret[k] if order[k] else yin[k]
        fresh = dot_tn(high, returned) + dot_tn(low, returned)
        mixed[...] = mixed[...] + fresh if combined else fresh
        combined.append(k)

    def prepare_sums():
        i, j = iota((BLOCK, BLOCK), 0), iota((BLOCK, BLOCK), 1)
        for level, h in enumerate(LEVELS):
            edge = (i & ~(2 * h - 1)) + h
            after = (j >= edge) & (j <= i)
            ahead = (j > i) & (j < edge)
            m = one_where(after | ahead).astype(BF16)
            sums[pl.ds(level * BLOCK, BLOCK), pl.ds(0, BLOCK)] = m
            sums[pl.ds(level * BLOCK, BLOCK), pl.ds(BLOCK, BLOCK)] = m
        for level, m in ((len(LEVELS), j <= i), (len(LEVELS) + 1, j > i)):
            m = one_where(m).astype(BF16)
            sums[pl.ds(level * BLOCK, BLOCK), pl.ds(0, BLOCK)] = m
            sums[pl.ds(level * BLOCK, BLOCK), pl.ds(BLOCK, BLOCK)] = m

    first_head = iota((BLOCK, BLOCK), 1) < BLOCK // 2

    def by_head(value):
        return jnp.concatenate([jnp.where(first_head, value, 0.0), jnp.where(first_head, 0.0, value)], axis=0).astype(BF16)

    def gla_block(b):
        if b == 0:
            for load in small[2:] + inputs[1:5]:
                load.wait()
        r = pl.ds(b * BLOCK, BLOCK)
        factors = jnp.concatenate([position_factor[:, r], extra_t[:, r], jnp.zeros((5, BLOCK), F32)], axis=0).T
        f = forget[r, :].astype(F32)
        g = (jnp.minimum(f, 0.0) - jnp.log1p(jnp.exp(-jnp.abs(f)))) * rate[...] * factors[:, 0:1]
        g = g + jnp.where(first_head, factors[:, 1:2], factors[:, 2:3])
        high = g.astype(BF16)
        low = (g - high.astype(F32)).astype(BF16)
        e = jnp.exp(dot(sums[...], jnp.concatenate([high, low], axis=0)))
        q, k = queries[r, :].astype(F32), keys[r, :].astype(F32)
        i, j = iota((BLOCK, 2 * BLOCK), 0), iota((BLOCK, 2 * BLOCK), 1) & (BLOCK - 1)
        apart = i ^ j
        scores = None
        for level, h in enumerate(LEVELS):
            factor = e[level * BLOCK : (level + 1) * BLOCK]
            s = dot_nt((q * factor).astype(BF16), by_head(k * factor))
            scores = s if scores is None else jnp.where(apart < 2 * h, s, scores)
        scores = jnp.where(apart < 1, dot_nt(queries[r, :], by_head(k)), scores)
        scores = jnp.where(i >= j, scores, 0.0).astype(BF16)
        n = len(LEVELS)
        from_start = e[n * BLOCK : (n + 1) * BLOCK]
        to_end = e[(n + 1) * BLOCK : (n + 2) * BLOCK]
        qg = q * from_start
        outs = [
            dot(scores[:, h * BLOCK : (h + 1) * BLOCK], values[r, pl.ds(h * BLOCK, BLOCK)]) for h in range(2)
        ]
        if b:
            carried = dot_nt(by_head(qg), state[...].astype(BF16))
            outs = [o + carried[h * BLOCK : (h + 1) * BLOCK] for h, o in enumerate(outs)]
            decayed_q[r, :] = (qg * total[...]).astype(BF16)
        else:
            decayed_q[r, :] = qg.astype(BF16)
        for h in range(2):
            local_out[r, pl.ds(h * BLOCK, BLOCK)] = outs[h]
        grown = dot_tn(values[r, :], (k * to_end).astype(BF16))
        fresh = jnp.where(first_head, grown[0:BLOCK], grown[BLOCK : 2 * BLOCK])
        through = from_start[BLOCK - 1 : BLOCK, :]
        if b:
            state[...] = state[...] * through + fresh
            total[...] = total[...] * through
        else:
            state[...] = fresh
            total[...] = through

    def packed(s, d):
        high = d.astype(BF16).astype(F32)
        row = iota((16, BLOCK), 0)
        tail = jnp.where(row == 0, high, jnp.where(row == 1, d - high, 0.0))
        return s.astype(BF16), tail.astype(BF16)

    def opened(ref, at):
        tail = ref[at, pl.ds(BLOCK, 16), :].astype(F32)
        return ref[at, pl.ds(0, BLOCK), :].astype(F32), tail[0:1] + tail[1:2]

    def states_y():
        s, tail = packed(state[...], total[...])
        tz[1, pl.ds(0, BLOCK), :] = s
        tz[1, pl.ds(BLOCK, 16), :] = tail

        def send(t, carry):
            to = lax.rem(yc + t, nyc)
            remote(tz.at[1], sy.at[yc], sys_, syr, at_yc(to)).start()
            return carry

        lax.fori_loop(1, nyc, send, 0)
        sy[yc, pl.ds(0, BLOCK), :] = s
        sy[yc, pl.ds(BLOCK, 16), :] = tail

    def states_z():
        arrived(sy.at[pl.ds(0, nyc - 1)], syr)
        run_s, run_d = jnp.zeros((BLOCK, BLOCK), F32), jnp.ones((1, BLOCK), F32)
        before[pl.ds(0, BLOCK), :] = run_s
        before[pl.ds(BLOCK, 8), :] = jnp.broadcast_to(run_d, (8, BLOCK))
        for s in range(nyc):
            new_s, new_d = opened(sy, s)
            run_s, run_d = run_s * new_d + new_s, run_d * new_d

            @pl.when(s < yc)
            def _(run_s=run_s, run_d=run_d):
                before[pl.ds(0, BLOCK), :] = run_s
                before[pl.ds(BLOCK, 8), :] = jnp.broadcast_to(run_d, (8, BLOCK))

        s, tail = packed(run_s, run_d)
        tz[0, pl.ds(0, BLOCK), :] = s
        tz[0, pl.ds(BLOCK, 16), :] = tail
        for d in range(1, nz):

            @pl.when(z + d < nz)
            def _(d=d):
                remote(tz.at[0], sz.at[z], szs.at[d], szr.at[z], {"z": z + d}).start()

    def states_in():
        incoming[...] = jnp.zeros((BLOCK, BLOCK), F32)
        for s in range(nz - 1):

            @pl.when(s < z)
            def _(s=s):
                arrived(sz.at[s], szr.at[s])
                new_s, new_d = opened(sz, s)
                incoming[...] = incoming[...] * new_d + new_s

        incoming[...] = incoming[...] * before[pl.ds(BLOCK, 8), :][0:1] + before[pl.ds(0, BLOCK), :]

    mrows = length // NX
    width_of_group = 2 * BLOCK

    def mix():
        s = incoming[...].astype(BF16)
        for b in range(blocks):
            r = pl.ds(b * BLOCK, BLOCK)
            carried = dot_nt(by_head(decayed_q[r, :].astype(F32)), s)
            for h in range(2):
                c = pl.ds(h * BLOCK, BLOCK)
                o = local_out[r, c] + carried[h * BLOCK : (h + 1) * BLOCK]
                o = o * lax.rsqrt(jnp.mean(o * o, axis=1, keepdims=True) + EPS) * head_gain[h : h + 1, :]
                normed[r, c] = o.astype(BF16)
        normed_all[:, 0:width_of_group] = normed[pl.ds(times(x, mrows), mrows), :]
        for r, to in ((1, right), (2, opposite), (3, left)):
            remote(
                normed.at[pl.ds(times(to, mrows), mrows), :],
                normed_all.at[:, pl.ds(r * width_of_group, width_of_group)],
                ms,
                mr.at[r],
                {"tp": to},
            ).start()

    piece = out_weight.shape[1] // nyc
    phalf = piece // 2
    above, below = lax.rem(y + 1, ny), lax.rem(y + ny - 1, ny)

    def piece_of(which, start, size):
        return pl.ds(pl.multiple_of((c * ny + which) * piece + start, 16), size)

    def weights_x():
        inputs[5].wait()
        here = piece_of(y, 0, piece)
        remote(out_weight.at[0, here], out_weight.at[1, here], ws, wr.at[0], {"tp": right}).start()
        remote(out_weight.at[0, here], out_weight.at[3, here], ws, wr.at[1], {"tp": left}).start()

    def weights_x_relay():
        here, a, b = piece_of(y, 0, piece), piece_of(y, 0, phalf), piece_of(y, phalf, phalf)
        arrived(out_weight.at[1, here], wr.at[0])
        remote(out_weight.at[1, a], out_weight.at[2, a], ws, wr.at[2], {"tp": right}).start()
        arrived(out_weight.at[3, here], wr.at[1])
        remote(out_weight.at[3, b], out_weight.at[2, b], ws, wr.at[3], {"tp": left}).start()

    others = pl.ds(1, NX - 1)

    def weights_y(r):
        here, a, b = piece_of(y, 0, piece), piece_of(y, 0, phalf), piece_of(y, phalf, phalf)
        if r == 2:
            arrived(out_weight.at[2, a], wr.at[2])
            arrived(out_weight.at[2, b], wr.at[3])
        if ny > 1:
            mine = out_weight.at[r, here]
            remote(mine, mine, ws, wr.at[4 * r], {"y": above}).start()
            remote(mine, mine, ws, wr.at[4 * r + 1], {"y": below}).start()

    def weights_y_relay(r):
        if ny > 1:
            arrived(out_weight.at[r, piece_of(below, 0, piece)], wr.at[4 * r])
            a = out_weight.at[r, piece_of(below, 0, phalf)]
            remote(a, a, ws, wr.at[4 * r + 2], {"y": above}).start()
            arrived(out_weight.at[r, piece_of(above, 0, piece)], wr.at[4 * r + 1])
            b = out_weight.at[r, piece_of(above, phalf, phalf)]
            remote(b, b, ws, wr.at[4 * r + 3], {"y": below}).start()

    def column_of(which):
        return out_weight.at[others, pl.ds(times(which * ny, piece), ny * piece)]

    def weights_c():
        if ny > 1:
            far = lax.rem(y + 2, ny)
            for r in range(1, NX):
                arrived(out_weight.at[r, piece_of(far, 0, phalf)], wr.at[4 * r + 2])
                arrived(out_weight.at[r, piece_of(far, phalf, phalf)], wr.at[4 * r + 3])
        if nc > 1:
            remote(column_of(c), column_of(c), ws, wr.at[4 * NX], {"c": 1 - c}).start()

    def mix_end():
        if nc > 1:
            arrived(column_of(1 - c), wr.at[4 * NX])
        for r in range(1, NX):
            arrived(normed_all.at[:, pl.ds(r * width_of_group, width_of_group)], mr.at[r])
        full = out_weight[...].reshape(NX * width_of_group, out_weight.shape[2])
        mix_held[...] = dot(normed_all[...], full).astype(BF16)
        pltpu.make_async_copy(mix_held, mix_out, output_sem.at[0]).start()

    def at(work):
        return lambda d: work(order.index(d))

    def alone(*works):
        def run(index):
            for work in works:
                work()

        return run

    does = {
        "ds": at(send_z),
        "fy": at(forward_y),
        "fx": at(forward_x),
        "rl": at(relay),
        "ex": expert,
        "ap": at(add_pass),
        "gy": at(give_back_y),
        "gz": at(give_back_z),
        "cb": at(combine),
        "gla": gla_block,
        "sy": alone(states_y),
        "sz": alone(states_z),
        "mx": alone(states_in, mix),
        "me": alone(mix_end),
        "wr": alone(weights_x_relay),
        "wy": weights_y,
        "wz": weights_y_relay,
        "wc": alone(weights_c),
    }
    for d in sorted(order, key=lambda d: min(d, nz - d)):
        dispatch(d)
    prepare_sums()
    pl.semaphore_wait(barrier, 3 + (nz - 1) + (nyc - 1))
    weights_x()
    for name, index in program_of(nz):
        does[name](index)
    moe_held[...] = mixed[...].astype(BF16)
    pltpu.make_async_copy(moe_held, moe_out, output_sem.at[1]).start()

    for q in sorted(set(quarters)):
        across = pl.ds(0, q * quarter)
        forwarded = quarters.count(q)
        sent = forwarded - (quarters[order.index(0)] == q)
        arrived(xq.at[pl.ds(0, forwarded * (zrows - CAP)), across], ys.at[q // 2])
        if sent:
            arrived(xq.at[pl.ds(0, sent * zrows), across], zs.at[q // 2])
    gathered, relayed = sum(q < 4 for q in quarters), sum(q < 2 for q in quarters)
    for side in range(2):
        if gathered:
            arrived(xq.at[pl.ds(0, gathered * zrows), columns(0)], xs.at[side])
        if relayed:
            arrived(xq.at[pl.ds(0, relayed * half), columns(0)], xs.at[2 + side])
        arrived(xq.at[pl.ds(0, nz * half), columns(0)], ps.at[side])
        arrived(xq.at[pl.ds(0, nz * zrows), columns(0)], ps.at[2 + side])
    arrived(xq.at[pl.ds(0, nz * (zrows - CAP)), columns(0)], y2s)
    if nz > 1:
        arrived(xq.at[pl.ds(0, (nz - 1) * zrows), columns(0)], z2s)
    arrived(sy.at[pl.ds(0, nyc - 1)], sys_)
    for d in range(1, nz):

        @pl.when(z + d < nz)
        def _(d=d):
            arrived(tz.at[0], szs.at[d])

    arrived(normed_all.at[:, pl.ds(0, (NX - 1) * width_of_group)], ms)
    sent = 2 * (piece + phalf) * (NX if ny > 1 else 1) + ((NX - 1) * ny * piece if nc > 1 else 0)
    arrived(out_weight.at[pl.ds(0, sent // out_weight.shape[1])], ws)
    pltpu.make_async_copy(mix_held, mix_out, output_sem.at[0]).wait()
    pltpu.make_async_copy(moe_held, moe_out, output_sem.at[1]).wait()


def body(
    nz,
    ny,
    nc,
    queries,
    key_rows,
    value_rows,
    forget_gate_input,
    channel_decay_rate,
    position_decay_factor,
    extra_log_decay,
    head_norm_gain,
    output_projection_weight,
    expert_input_rows,
    expert_norm_gain,
    routes,
    chosen_expert_weights,
    expert_gate_weight,
    expert_up_weight,
    expert_down_weight,
):
    length, channels = queries.shape
    tokens, width = expert_input_rows.shape
    hidden = expert_gate_weight.shape[2]
    quarter = width // NX
    nyc = ny * nc
    zrows = nyc * CAP
    dma, vmem = pltpu.SemaphoreType.DMA, pltpu.VMEM
    mrows = length // NX
    outs = pl.pallas_call(
        functools.partial(kernel, nz, ny, nc),
        out_shape=(
            jax.ShapeDtypeStruct((mrows, width), BF16),
            jax.ShapeDtypeStruct((tokens, quarter), BF16),
        ),
        in_specs=[pl.BlockSpec(memory_space=pl.ANY)] * 16,
        out_specs=(pl.BlockSpec(memory_space=pl.ANY), pl.BlockSpec(memory_space=pl.ANY)),
        scratch_shapes=[
            vmem((routes.shape[1], tokens), routes.dtype),
            vmem((routes.shape[1], tokens), F32),
            vmem((1, width), F32),
            vmem((1, channels), F32),
            vmem((1, length), F32),
            vmem((extra_log_decay.shape[1], length), F32),
            vmem(head_norm_gain.shape, F32),
            vmem((tokens, width), BF16),
            vmem((length, channels), BF16),
            vmem((length, channels), BF16),
            vmem((length, value_rows.shape[1]), BF16),
            vmem((length, channels), BF16),
            vmem((NX, *output_projection_weight.shape), BF16),
            dma((7,)),
            dma((6,)),
            vmem((mrows, width), BF16),
            vmem((tokens, quarter), BF16),
            vmem((tokens, quarter), F32),
            dma((2,)),
            vmem((width, hidden), BF16),
            vmem((width, hidden), BF16),
            vmem((hidden, width), BF16),
            dma((3,)),
            vmem((nz, zrows, width), BF16),
            vmem((nz, zrows, width), BF16),
            vmem((nz * zrows, width), BF16),
            vmem((nz * zrows, width), BF16),
            vmem((nz, zrows // 2, quarter), BF16),
            vmem((nz, zrows // 2, quarter), BF16),
            vmem((nz * zrows, quarter), BF16),
            vmem((nz * zrows, quarter), BF16),
            vmem((nz * zrows, quarter), BF16),
            vmem((nz, zrows, quarter), BF16),
            vmem((nz, zrows, quarter), BF16),
            dma((3,)),
            dma((nz,)),
            dma((3,)),
            dma((nz,)),
            dma((4,)),
            dma((4, nz)),
            dma((4,)),
            dma((4, nz)),
            dma(()),
            dma((nz,)),
            dma(()),
            dma((nz,)),
            vmem(((len(LEVELS) + 2) * BLOCK, 2 * BLOCK), BF16),
            vmem((length, 2 * BLOCK), F32),
            vmem((length, BLOCK), BF16),
            vmem((BLOCK, BLOCK), F32),
            vmem((1, BLOCK), F32),
            vmem((length, 2 * BLOCK), BF16),
            vmem((nyc, BLOCK + 16, BLOCK), BF16),
            vmem((2, BLOCK + 16, BLOCK), BF16),
            vmem((nz, BLOCK + 16, BLOCK), BF16),
            vmem((BLOCK, BLOCK), F32),
            vmem((BLOCK + 8, BLOCK), F32),
            dma(()),
            dma(()),
            dma((nz,)),
            dma((nz,)),
            vmem((mrows, NX * value_rows.shape[1]), BF16),
            dma(()),
            dma((NX,)),
            dma(()),
            dma((4 * NX + 1,)),
        ],
        compiler_params=pltpu.CompilerParams(
            collective_id=0, has_side_effects=True, vmem_limit_bytes=60 * 1024 * 1024
        ),
        name="mixer_and_experts",
    )(
        routes.T,
        chosen_expert_weights.T,
        expert_norm_gain[None, :],
        channel_decay_rate[None, :],
        position_decay_factor[None, :],
        extra_log_decay.T,
        head_norm_gain,
        expert_input_rows,
        queries,
        key_rows,
        value_rows,
        forget_gate_input,
        output_projection_weight,
        expert_gate_weight,
        expert_up_weight,
        expert_down_weight,
    )
    return pl.pallas_call(
        handed_over,
        out_shape=tuple(jax.ShapeDtypeStruct(o.shape, o.dtype) for o in outs),
        in_specs=[pl.BlockSpec(memory_space=vmem)] * 2,
        out_specs=(pl.BlockSpec(memory_space=vmem),) * 2,
        name="handed_over",
    )(*outs)


def handed_over(mix_in, moe_in, mix_out, moe_out):
    mix_out[...] = mix_in[...]
    moe_out[...] = moe_in[...]


def mapped(mesh, nz, ny, nc):
    finer = Mesh(mesh.devices.reshape(nz, ny, nc, NX), EP_TP)
    return jax.shard_map(
        functools.partial(body, nz, ny, nc),
        mesh=finer,
        in_specs=(
            P(EP, "tp"),
            P(EP, "tp"),
            P(EP, "tp"),
            P(EP, "tp"),
            P("tp"),
            P(EP),
            P(EP, "tp"),
            P("tp", None),
            P("tp", None),
            P(EP, None),
            P(),
            P(EP, None),
            P(EP, None),
            P(EP, None, "tp"),
            P(EP, None, "tp"),
            P(EP, "tp", None),
        ),
        out_specs=(P(EP_TP, None), P(EP, "tp")),
        check_vma=False,
    )


def solution(mesh):
    return mapped(mesh, 8, 4, 2)
```
